32 devices in a mesh: sp: 8 (over z, y), tp: 4 (over x, core).
Axes of the slice: x: 2, y: 2, z: 4, core: 2. Of those that a mesh axis runs over, the one named last changes fastest.
Arguments:
- tokens: bfloat16 [4096, 2048], P('sp', 'tp'), may hold values from -6 to 6
- norm_gain: float32 [2048], replicated, may hold values from 0.1 to 1.9
- query_weight: bfloat16 [2048, 2048], P('sp', 'tp'), may hold values from -0.125 to 0.125
- key_weight: bfloat16 [2048, 512], P('sp', 'tp'), may hold values from -0.125 to 0.125
- value_weight: bfloat16 [2048, 512], P('sp', 'tp'), may hold values from -0.125 to 0.125
- pool_in_weight: bfloat16 [2048, 1024], P('sp', 'tp'), may hold values from -0.125 to 0.125
- pool_mix_weight: bfloat16 [4, 256, 256], P('tp'), may hold values from -0.375 to 0.375
- sink_logit: float32 [32], P('tp'), may hold values from -300 to 300
- out_pool_weight: bfloat16 [1024, 2048], P('tp', 'sp'), may hold values from -0.109375 to 0.109375
- out_attn_weight: bfloat16 [2048, 2048], P('tp', 'sp'), may hold values from -1.25 to 1.25
Outputs:
- mixed: bfloat16 [4096, 2048], P('sp', 'tp')
- log_weight: float32 [32, 4096], P('tp', 'sp')
The draws below stay inside these ranges and needn't reach their ends.
All inputs are finite; a program needn't handle non-finite values.
Results may differ from the reference program's by a relative error of at most 0.012.
Values may be sent and summed in bfloat16 or wider, within the bound.
A program may use at most 64 MiB of HBM per device.

```python
import jax
import jax.numpy as jnp
from jax import lax

D = 2048
HQ = 32
KVH = 8
HD = 64
GROUPS = 4
POOL_GC = 256
WINDOW = 128
GRID_W = 64
POOL_WIDTH = 1024
TOKENS = 4096
N_TP = 4


def draw_sink_logit(key, part):
    heads_per_group = HQ // KVH
    drawn = jax.random.uniform(jax.random.fold_in(key, 11), (KVH, heads_per_group), jnp.float32, 2.0, 6.0)
    return drawn.reshape(HQ)


def block_scale(key, shape, cuts, low, largest):
    gain, own = 1.0, jax.random.fold_in(key, 6)
    for position, parts in cuts:
        heights = jnp.exp(jax.random.uniform(jax.random.fold_in(own, position), (parts,), jnp.float32, low / len(cuts), largest / len(cuts)))
        gain = gain * jnp.repeat(heights, shape[position] // parts).reshape([-1 if axis == position else 1 for axis in range(len(shape))])
    return gain


def scatter_about(stream_key, dims, spread, bound, pieces=(), kind=jnp.bfloat16):
    values = jax.random.normal(stream_key, dims, jnp.float32) * spread
    if len(pieces) > 0:
        values = block_scale(stream_key, dims, pieces, -0.22, 0.18) * values
    return jnp.clip(values, min=-bound, max=bound).astype(kind)


def setup_inputs(seed: int = 0) -> dict:
    streams_of = jax.random.split(jax.random.key(seed), 11)
    tokens = scatter_about(streams_of[0], (TOKENS, D), 1.0, 6.0, ((0, 8), (1, 4)))
    norm_gain = jnp.clip(1.0 + 0.18 * jax.random.normal(streams_of[1], (D,), jnp.float32), 0.1, 1.9)
    query_weight = scatter_about(streams_of[2], (D, HQ * HD), D ** -0.5, 0.125, ((0, 8), (1, 4)))
    key_weight = scatter_about(streams_of[3], (D, KVH * HD), D ** -0.5, 0.125, ((0, 8), (1, 4)))
    value_weight = scatter_about(streams_of[4], (D, KVH * HD), D ** -0.5, 0.125, ((0, 8), (1, 4)))
    pool_in_weight = scatter_about(streams_of[5], (D, POOL_WIDTH), D ** -0.5, 0.125, ((0, 8), (1, 4)))
    pool_mix_weight = scatter_about(streams_of[6], (GROUPS, POOL_GC, POOL_GC), POOL_GC ** -0.5, 0.375, ((0, 4),))
    sink_logit = draw_sink_logit(jax.random.fold_in(streams_of[10], 71), 0)
    out_pool_weight = scatter_about(streams_of[8], (POOL_WIDTH, D), (POOL_WIDTH + HQ * HD) ** -0.5, 0.109375, ((0, 4), (1, 8)))
    out_attn_weight = scatter_about(streams_of[9], (HQ * HD, D), ((POOL_WIDTH + HQ * HD) // 144) ** -0.5, 1.25, ((0, 4), (1, 8)))
    return {"tokens": tokens, "norm_gain": norm_gain, "query_weight": query_weight, "key_weight": key_weight, "value_weight": value_weight, "pool_in_weight": pool_in_weight, "pool_mix_weight": pool_mix_weight, "sink_logit": sink_logit, "out_pool_weight": out_pool_weight, "out_attn_weight": out_attn_weight}


norm_eps = 1e-06
rope_base = 10000.0
pool_reach = 8
neg_fill = -1e+30

def rope_tables(positions, head_dim):
    n_freq = head_dim // 4
    freqs = rope_base ** (-jnp.arange(n_freq, dtype=jnp.float32) / n_freq)
    rows = (positions // GRID_W).astype(jnp.float32)
    columns = (positions % GRID_W).astype(jnp.float32)
    row_angle = rows[:, None] * freqs[None, :]
    col_angle = columns[:, None] * freqs[None, :]
    return (jnp.cos(row_angle), jnp.sin(row_angle), jnp.cos(col_angle), jnp.sin(col_angle))

def rotate_half(values, cosine, sine):
    middle = values.shape[-1] // 2
    first = values[..., :middle]
    second = values[..., middle:]
    return jnp.concatenate([first * cosine - second * sine, second * cosine + first * sine], -1)

def rotate_heads(values, tables, head_dim):
    rows_count = values.shape[0]
    shaped = values.astype(jnp.float32).reshape(rows_count, -1, head_dim)
    cos_r, sin_r, cos_c, sin_c = [table[:, None, :] for table in tables]
    split = head_dim // 2
    turned = jnp.concatenate([rotate_half(shaped[..., :split], cos_r, sin_r), rotate_half(shaped[..., split:], cos_c, sin_c)], -1)
    return turned.reshape(rows_count, -1).astype(jnp.bfloat16)

def pool_group(extended, own, positions, half_width, seq_total):
    rows_count = own.shape[0]
    summed = jnp.zeros(own.shape, jnp.float32)
    counted = jnp.zeros((rows_count,), jnp.float32)
    for shift_by in range(-pool_reach, pool_reach):
        source = positions + shift_by
        inside = (shift_by >= -half_width) & (shift_by < half_width) & (source >= 0) & (source < seq_total)
        window_rows = extended[pool_reach + shift_by:pool_reach + shift_by + rows_count].astype(jnp.float32)
        summed = summed + jnp.where(inside[:, None], window_rows, 0.0)
        counted = counted + inside.astype(jnp.float32)
    return (summed / counted[:, None] - own.astype(jnp.float32)).astype(jnp.bfloat16)

def attend_block(queries, keys, values, sink, query_pos, key_pos, seq_total):
    scores = jnp.einsum('qhgd,khd->hgqk', queries.astype(jnp.float32), keys.astype(jnp.float32)) * HD ** (-0.5)
    valid = (jnp.abs(query_pos[:, None] - key_pos[None, :]) <= WINDOW) & (key_pos >= 0)[None, :] & (key_pos < seq_total)[None, :]
    scores = jnp.where(valid, scores, neg_fill)
    row_top = jnp.maximum(lax.optimization_barrier(jnp.max(scores, -1)), sink[:, :, None])
    exps = jnp.exp(scores - row_top[..., None])
    row_total = lax.optimization_barrier(jnp.sum(exps, -1)) + jnp.exp(sink[:, :, None] - row_top)
    weights = (exps / row_total[..., None]).astype(jnp.bfloat16)
    attended = jnp.einsum('hgqk,khd->qhgd', weights.astype(jnp.float32), values.astype(jnp.float32))
    return (attended.astype(jnp.bfloat16), row_top + jnp.log(row_total))

def reference(tokens, norm_gain, query_weight, key_weight, value_weight, pool_in_weight, pool_mix_weight, sink_logit, out_pool_weight, out_attn_weight):
    seq_total = tokens.shape[0]
    wide = tokens.astype(jnp.float32)
    normed = (wide * lax.rsqrt(lax.optimization_barrier(jnp.mean(wide * wide, -1, keepdims=True)) + norm_eps) * norm_gain).astype(jnp.bfloat16)
    query = jnp.dot(normed, query_weight, preferred_element_type=jnp.float32).astype(jnp.bfloat16)
    key = jnp.dot(normed, key_weight, preferred_element_type=jnp.float32).astype(jnp.bfloat16)
    value = jnp.dot(normed, value_weight, preferred_element_type=jnp.float32).astype(jnp.bfloat16)
    pool_input = jnp.dot(normed, pool_in_weight, preferred_element_type=jnp.float32).astype(jnp.bfloat16)
    positions = jnp.arange(seq_total, dtype=jnp.int32)
    tables = rope_tables(positions, HD)
    rot_query = rotate_heads(query, tables, HD)
    rot_key = rotate_heads(key, tables, HD)
    pool_parts = []
    for group in range(GROUPS):
        own = pool_input[:, group * POOL_GC:(group + 1) * POOL_GC]
        extended = jnp.pad(own, ((pool_reach, pool_reach), (0, 0)))
        pooled = pool_group(extended, own, positions, 2 ** group, seq_total)
        pool_parts.append(jnp.dot(pooled, pool_mix_weight[group], preferred_element_type=jnp.float32).astype(jnp.bfloat16))
    pool_out = jnp.concatenate(pool_parts, 1)
    grp = HQ // KVH
    query_heads = rot_query.reshape(seq_total, KVH, grp, HD)
    key_pad = jnp.pad(rot_key.reshape(seq_total, KVH, HD), ((WINDOW, WINDOW), (0, 0), (0, 0)))
    value_pad = jnp.pad(value.reshape(seq_total, KVH, HD), ((WINDOW, WINDOW), (0, 0), (0, 0)))
    sink = sink_logit.reshape(KVH, grp)
    block_rows = 512

    def block_fn(block_index):
        start = (block_index * block_rows).astype(jnp.int32)
        queries = lax.dynamic_slice_in_dim(query_heads, start, block_rows, 0)
        keys = lax.dynamic_slice_in_dim(key_pad, start, block_rows + 2 * WINDOW, 0)
        values = lax.dynamic_slice_in_dim(value_pad, start, block_rows + 2 * WINDOW, 0)
        query_pos = start + jnp.arange(block_rows, dtype=jnp.int32)
        key_pos = start - WINDOW + jnp.arange(block_rows + 2 * WINDOW, dtype=jnp.int32)
        return attend_block(queries, keys, values, sink, query_pos, key_pos, seq_total)
    n_blocks = seq_total // block_rows
    attended, log_blocks = lax.map(block_fn, jnp.arange(n_blocks, dtype=jnp.int32))
    attended = attended.reshape(seq_total, HQ * HD)
    log_weight = jnp.moveaxis(log_blocks.reshape(n_blocks, HQ, block_rows), 0, 1).reshape(HQ, seq_total)
    attn_group = HQ * HD // N_TP
    mixed = jnp.zeros((seq_total, D), jnp.float32)
    for part in range(N_TP):
        term = jnp.dot(pool_out[:, part * POOL_GC:(part + 1) * POOL_GC], out_pool_weight[part * POOL_GC:(part + 1) * POOL_GC], preferred_element_type=jnp.float32)
        term = term + jnp.dot(attended[:, part * attn_group:(part + 1) * attn_group], out_attn_weight[part * attn_group:(part + 1) * attn_group], preferred_element_type=jnp.float32)
        rounded = lax.optimization_barrier(term.astype(jnp.bfloat16))
        mixed = mixed + rounded.astype(jnp.float32)
    return (mixed.astype(jnp.bfloat16), log_weight)
```

```python
import functools
import math

import jax
import jax.numpy as jnp
from jax import lax
from jax.experimental import pallas as pl
from jax.experimental.pallas import tpu as pltpu
from jax.sharding import PartitionSpec as P

HD = 64
WINDOW = 128
GRID_W = 64


norm_eps = 1e-06
rope_base = 10000.0
pool_reach = 8
neg_fill = -1e30


def with_halo(cells, sides, width):
    for axis, dim in sides:
        count = lax.axis_size(axis)
        ends = count - 1
        head = lax.slice_in_dim(cells, 0, width, axis=dim)
        tail = lax.slice_in_dim(cells, cells.shape[dim] - width, cells.shape[dim], axis=dim)
        cells = jnp.concatenate(
            [
                lax.ppermute(tail, axis, [(i, (i + 1) % count) for i in range(ends)]),
                cells,
                lax.ppermute(head, axis, [((i + 1) % count, i) for i in range(ends)]),
            ],
            axis=dim,
        )
    return cells


def rope_tables(positions, head_dim):
    n_freq = head_dim // 4
    freqs = rope_base ** (-jnp.arange(n_freq, dtype=jnp.float32) / n_freq)
    rows = (positions // GRID_W).astype(jnp.float32)
    columns = (positions % GRID_W).astype(jnp.float32)
    row_angle = rows[:, None] * freqs[None, :]
    col_angle = columns[:, None] * freqs[None, :]
    return (jnp.cos(row_angle), jnp.sin(row_angle), jnp.cos(col_angle), jnp.sin(col_angle))


def rotate_half(values, cosine, sine):
    middle = values.shape[-1] // 2
    first = values[..., :middle]
    second = values[..., middle:]
    return jnp.concatenate([first * cosine - second * sine, second * cosine + first * sine], -1)


def rotate_heads(values, tables, head_dim):
    rows_count = values.shape[0]
    shaped = values.astype(jnp.float32).reshape(rows_count, -1, head_dim)
    cos_r, sin_r, cos_c, sin_c = [table[:, None, :] for table in tables]
    split = head_dim // 2
    turned = jnp.concatenate(
        [
            rotate_half(shaped[..., :split], cos_r, sin_r),
            rotate_half(shaped[..., split:], cos_c, sin_c),
        ],
        -1,
    )
    return turned.reshape(rows_count, -1).astype(jnp.bfloat16)


def pool_group(extended, own, positions, half_width, seq_total):
    rows_count = own.shape[0]
    summed = jnp.zeros(own.shape, jnp.float32)
    counted = jnp.zeros((rows_count,), jnp.float32)
    for shift_by in range(-pool_reach, pool_reach):
        source = positions + shift_by
        inside = (
            (shift_by >= -half_width)
            & (shift_by < half_width)
            & (source >= 0)
            & (source < seq_total)
        )
        window_rows = extended[pool_reach + shift_by : pool_reach + shift_by + rows_count].astype(
            jnp.float32
        )
        summed = summed + jnp.where(inside[:, None], window_rows, 0.0)
        counted = counted + inside.astype(jnp.float32)
    return (summed / counted[:, None] - own.astype(jnp.float32)).astype(jnp.bfloat16)


def attend_block(queries, keys, values, sink, query_pos, key_pos, seq_total):
    scores = jnp.einsum(
        "qhgd,khd->hgqk", queries, keys, preferred_element_type=jnp.float32
    ) * HD ** (-0.5)
    valid = (
        (jnp.abs(query_pos[:, None] - key_pos[None, :]) <= WINDOW)
        & (key_pos >= 0)[None, :]
        & (key_pos < seq_total)[None, :]
    )
    scores = jnp.where(valid, scores, neg_fill)
    row_top = jnp.maximum(jnp.max(scores, -1), sink[:, :, None])
    exps = jnp.exp(scores - row_top[..., None])
    row_total = jnp.sum(exps, -1) + jnp.exp(sink[:, :, None] - row_top)
    weights = (exps / row_total[..., None]).astype(jnp.bfloat16)
    attended = jnp.einsum("hgqk,khd->qhgd", weights, values, preferred_element_type=jnp.float32)
    return (attended.astype(jnp.bfloat16), row_top + jnp.log(row_total))


def fetch_outputs(out_pool_weight, out_attn_weight):
    return (
        lax.all_gather(out_pool_weight, "sp", axis=1, tiled=True),
        lax.all_gather(out_attn_weight, "sp", axis=1, tiled=True),
    )


def local(
    tokens,
    norm_gain,
    query_weight,
    key_weight,
    value_weight,
    pool_in_weight,
    pool_mix_weight,
    sink_logit,
    out_pool_weight,
    out_attn_weight,
):
    whole = lax.all_gather(tokens, "tp", axis=1, tiled=True)
    wide = whole.astype(jnp.float32)
    normed = (
        wide * lax.rsqrt(jnp.mean(wide * wide, -1, keepdims=True) + norm_eps) * norm_gain
    ).astype(jnp.bfloat16)
    tok_rows = normed.shape[0]
    seq_total = tok_rows * lax.axis_size("sp")
    offset = lax.axis_index("sp") * tok_rows
    weights_in = (query_weight, key_weight, value_weight, pool_in_weight)
    pieces = (
        lax.all_gather(weights_in[0], "sp", axis=0, tiled=True),
        lax.all_gather(weights_in[1], "sp", axis=0, tiled=True),
        lax.all_gather(weights_in[2], "sp", axis=0, tiled=True),
        lax.all_gather(weights_in[3], "sp", axis=0, tiled=True),
    )
    sums = tuple((jnp.dot(normed, piece, preferred_element_type=jnp.float32) for piece in pieces))
    query, key, value, pool_input = [total.astype(jnp.bfloat16) for total in sums]
    positions = offset + jnp.arange(tok_rows, dtype=jnp.int32)
    tables = rope_tables(positions, HD)
    rot_query = rotate_heads(query, tables, HD)
    rot_key = rotate_heads(key, tables, HD)
    key_width = rot_key.shape[1]
    pool_ext = with_halo(pool_input, (("sp", 0),), pool_reach)
    pair_ext = with_halo(jnp.concatenate([rot_key, value], 1), (("sp", 0),), WINDOW)
    key_ext = pair_ext[:, :key_width]
    value_ext = pair_ext[:, key_width:]
    half_width = jnp.left_shift(jnp.int32(1), lax.axis_index("tp"))
    pooled = pool_group(pool_ext, pool_input, positions, half_width, seq_total)
    pool_out = jnp.dot(pooled, pool_mix_weight[0], preferred_element_type=jnp.float32).astype(
        jnp.bfloat16
    )
    heads_local = rot_query.shape[1] // HD
    kv_local = key_width // HD
    grp = heads_local // kv_local
    query_heads = rot_query.reshape(tok_rows, kv_local, grp, HD)
    key_heads = key_ext.reshape(-1, kv_local, HD)
    value_heads = value_ext.reshape(-1, kv_local, HD)
    sink = sink_logit.reshape(kv_local, grp)
    block_rows = min(tok_rows, 256)
    attended_parts = []
    log_parts = []
    for block_index in range(tok_rows // block_rows):
        start = block_index * block_rows
        query_pos = offset + start + jnp.arange(block_rows, dtype=jnp.int32)
        key_pos = offset + start - WINDOW + jnp.arange(block_rows + 2 * WINDOW, dtype=jnp.int32)
        attended_block, log_block = attend_block(
            query_heads[start : start + block_rows],
            key_heads[start : start + block_rows + 2 * WINDOW],
            value_heads[start : start + block_rows + 2 * WINDOW],
            sink,
            query_pos,
            key_pos,
            seq_total,
        )
        attended_parts.append(attended_block.reshape(block_rows, heads_local * HD))
        log_parts.append(log_block.reshape(heads_local, block_rows))
    attended = jnp.concatenate(attended_parts, 0)
    log_weight = jnp.concatenate(log_parts, 1)
    out_pool_full, out_attn_full = fetch_outputs(out_pool_weight, out_attn_weight)
    term = jnp.dot(pool_out, out_pool_full, preferred_element_type=jnp.float32)
    term = term + jnp.dot(attended, out_attn_full, preferred_element_type=jnp.float32)
    mixed = lax.psum_scatter(term.astype(jnp.bfloat16), "tp", scatter_dimension=1, tiled=True)
    return (mixed, log_weight)


NY = 2
NX = 2
CORES = 2
HALVES = 2
MESH = pl.DeviceIdType.MESH


def layer_kernel(
    nz,
    ntp,
    tok_ref,
    gain_ref,
    qw_ref,
    kw_ref,
    vw_ref,
    pw_ref,
    mix_ref,
    sink_ref,
    ow_ref,
    aw_ref,
    mixed_ref,
    log_ref,
    xg,
    normed,
    wg,
    wo,
    qrot,
    ext,
    act,
    part,
    rs1,
    tot,
    fin,
    cos_ref,
    sin_ref,
    mixb,
    sink_own,
    sinkb,
    log_own,
    log_in,
    load_send,
    load_recv,
    w_send,
    w_recv,
    x_loc,
    x_send,
    x_recv,
    xr_send,
    m_send,
    m_recv,
    h_send,
    h_recv,
    r1_send,
    r1_recv,
    r2_send,
    r2_recv,
):
    sp, tp = lax.axis_index("sp"), lax.axis_index("tp")
    z, y = sp // NY, sp % NY
    x, c = tp // CORES, tp % CORES
    nsp = nz * NY
    block_of = z * NY + c
    group_of = x * CORES + y
    straight = c == y
    crossed = c != y
    rows, width = tok_ref.shape
    brow = qw_ref.shape[0]
    qn, kn, pn = qw_ref.shape[1], kw_ref.shape[1], pw_ref.shape[1]
    heads, kv_local = qn // HD, kn // HD
    grp = heads // kv_local
    gw = 2 * kn
    groups = wg.shape[0]
    pool_rows = ow_ref.shape[0]
    ohalf = wo.shape[3]
    seq_total = rows * nsp
    per_owner = nsp // ntp
    pieces = groups + HALVES

    def at(zz, yy, xx, cc):
        return (zz * NY + yy, xx * CORES + cc)

    def remote(src, dst, send, recv, target):
        return pltpu.make_async_remote_copy(
            src_ref=src,
            dst_ref=dst,
            send_sem=send,
            recv_sem=recv,
            device_id=target,
            device_id_type=MESH,
        )

    sibling = at(z, y, x, 1 - c)
    partner = at(z, 1 - y, x, 1 - c)

    def shard_rows(block):
        return pl.ds(pl.multiple_of(block * brow, brow), brow)

    def load_parts(p, block):
        if p == 0:
            return [
                (kw_ref, wg.at[0, shard_rows(block), pl.ds(0, kn)]),
                (vw_ref, wg.at[0, shard_rows(block), pl.ds(kn, kn)]),
            ]
        if p == 2:
            return [(pw_ref, wg.at[2, shard_rows(block)])]
        if p < groups:
            return [(qw_ref.at[:, pl.ds((p // 2) * gw, gw)], wg.at[p, shard_rows(block)])]
        h = p - groups
        cols = pl.ds(h * ohalf, ohalf)
        return [
            (ow_ref.at[:, cols], wo.at[block, h, pl.ds(0, pool_rows)]),
            (aw_ref.at[:, cols], wo.at[block, h, pl.ds(pool_rows, wo.shape[2] - pool_rows)]),
        ]

    def load_local(p):
        return [
            pltpu.make_async_copy(a, b, load_recv.at[p, k])
            for k, (a, b) in enumerate(load_parts(p, sp))
        ]

    def load_swap(p):
        return [
            remote(a, b, load_send.at[p, k], load_recv.at[p, k], partner)
            for k, (a, b) in enumerate(load_parts(p, sp))
        ]

    def load_wait(p):
        @pl.when(straight)
        def _():
            for copy in load_local(p):
                copy.wait()

        @pl.when(crossed)
        def _():
            for k, (_, b) in enumerate(load_parts(p, block_of)):
                remote(b, b, load_send.at[p, k], load_recv.at[p, k], partner).wait_recv()

    onward = (z + 1 < nz, z >= 1)
    behind = (z, nz - 1 - z)

    def w_copy(p, block, way):
        ref = wg.at[p, shard_rows(block)] if p < groups else wo.at[block, p - groups]
        target = (at(z + 1, y, x, c), at(z - 1, y, x, c), sibling)[way]
        return remote(ref, ref, w_send.at[way, p, block], w_recv.at[p, block], target)

    def issue(copy, done):
        if done:
            copy.wait_send()
        else:
            copy.start()

    def send_own(p, ways, done=False):
        for way in ways:
            if way == 2:
                issue(w_copy(p, block_of, 2), done)
            else:

                @pl.when(onward[way])
                def _():
                    issue(w_copy(p, block_of, way), done)

    def relay(d, p, done=False):
        for way in range(2):
            source = (z - d, z + d)[way]
            block = source * NY + c

            @pl.when((source >= 0) & (source < nz))
            def _():
                if not done:
                    w_copy(p, block, 2).wait_recv()

                @pl.when(onward[way])
                def _():
                    issue(w_copy(p, block, way), done)

                issue(w_copy(p, block, 2), done)

    def stage(low, high):
        for total in range(low, high):
            for d in range(min(total, nz - 1) + 1):
                p = total - d
                if p < groups:
                    if d == 0:
                        load_wait(p)
                        send_own(p, (0, 1, 2))
                    else:
                        relay(d, p)

    def gathered(p):
        for source in range(nz):
            w_copy(p, source * NY + (1 - c), 2).wait_recv()

    cut = rows // 4
    spans = (pl.ds(0, cut), pl.ds(cut, rows - cut))

    def token_copy(kind, r):
        target = (at(z, y, x, y), at(z, y, 1 - x, y), at(z, 1 - y, x, y))[kind]
        return remote(
            tok_ref.at[spans[r]], xg.at[tp, spans[r]], x_send.at[kind, r], x_recv.at[tp, r], target
        )

    token_local = pltpu.make_async_copy(tok_ref, xg.at[tp], x_loc)

    def token_relay(k, r):
        slot = ((1 - x) if r == 0 else x) * CORES + k
        target = at(z, 1 - y, x, c) if r == 0 else at(z, y, 1 - x, c)
        ref = xg.at[slot, spans[r]]
        return remote(ref, ref, xr_send.at[k], x_recv.at[slot, r], target)

    def token_wait(slot, r):
        ref = xg.at[slot, spans[r]]
        remote(ref, ref, xr_send.at[0], x_recv.at[slot, r], sibling).wait_recv()

    mix_local = pltpu.make_async_copy(mix_ref.at[0], mixb, m_recv.at[0])
    mix_swap = remote(mix_ref.at[0], mixb, m_send.at[0], m_recv.at[0], partner)
    sink_swap = remote(sink_own, sinkb, m_send.at[1], m_recv.at[1], partner)

    @pl.when(straight)
    def _():
        for p in range(groups):
            for copy in load_local(p):
                copy.start()
        token_local.start()

    for head in range(heads):
        sink_own[head : head + 1, :] = jnp.full((1, 128), sink_ref[head], jnp.float32)

    @pl.when(straight)
    def _():
        sinkb[...] = sink_own[...]

    barrier = pltpu.get_barrier_semaphore()
    met = jnp.int32(0)
    for flip in range(1, NY * NX * CORES):
        fy, fx, fc = flip // 4, (flip // 2) % 2, flip % 2
        pl.semaphore_signal(
            barrier,
            inc=1,
            device_id=at(
                z,
                1 - y if fy else y,
                1 - x if fx else x,
                1 - c if fc else c,
            ),
            device_id_type=MESH,
        )
        met = met + 1
    for ok, zz in ((onward[0], z + 1), (onward[1], z - 1)):
        met = met + CORES * ok.astype(jnp.int32)

        @pl.when(ok)
        def _():
            for cc in range(CORES):
                pl.semaphore_signal(
                    barrier, inc=1, device_id=at(zz, y, x, cc), device_id_type=MESH
                )

    pl.semaphore_wait(barrier, met)

    @pl.when(straight)
    def _():
        for kind in (1, 2):
            for r in range(2):
                token_copy(kind, r if kind == 1 else 1 - r).start()
        mix_local.start()
        for p in range(groups, pieces):
            for copy in load_local(p):
                copy.start()

    @pl.when(crossed)
    def _():
        for copy in load_swap(0):
            copy.start()
        token_copy(2, 1).start()
        for r in range(2):
            token_copy(1, r).start()
            token_copy(0, r).start()
        for p in range(1, groups):
            for copy in load_swap(p):
                copy.start()
        token_copy(2, 0).start()
        sink_swap.start()
        mix_swap.start()
        for p in range(groups, pieces):
            for copy in load_swap(p):
                copy.start()

    stage(0, 1)
    ext[...] = jnp.zeros_like(ext)

    half = HD // 4
    lane = lax.broadcasted_iota(jnp.int32, (rows, 128), 1)
    is_first = (lane % (2 * half)) < half
    position = block_of * rows + lax.broadcasted_iota(jnp.int32, (rows, 128), 0)
    place = jnp.where((lane % HD) < 2 * half, position // GRID_W, position % GRID_W)
    freqs = jnp.exp((lane % half).astype(jnp.float32) * (-math.log(rope_base) / half))
    angle = place.astype(jnp.float32) * freqs
    cos_ref[...] = jnp.cos(angle)
    sine = jnp.sin(angle)
    sin_ref[...] = jnp.where(is_first, -sine, sine)

    stage(1, 2)
    for k in range(CORES):
        for r, ok in ((0, straight), (1, crossed)):

            @pl.when(ok)
            def _():
                token_relay(k, r).wait_recv()
                token_relay(k, r).start()

    stage(2, nz)

    @pl.when(straight)
    def _():
        token_local.wait()
        for r in range(2):
            token_wait(x * CORES + (1 - c), r)
        for k in range(CORES):
            token_wait((1 - x) * CORES + k, 1)

    @pl.when(crossed)
    def _():
        for k in range(CORES):
            token_wait(x * CORES + k, 0)
            for r in range(2):
                token_wait((1 - x) * CORES + k, r)

    norm_rows = 64

    @pl.loop(0, rows // norm_rows)
    def _(i):
        take = pl.ds(pl.multiple_of(i * norm_rows, norm_rows), norm_rows)
        pieces_in = [xg[t, take, :].astype(jnp.float32) for t in range(ntp)]
        total = sum(jnp.sum(piece * piece, -1, keepdims=True) for piece in pieces_in)
        scale = lax.rsqrt(total / (width * ntp) + norm_eps)
        for t in range(ntp):
            cols = pl.ds(t * width, width)
            normed[take, cols] = (pieces_in[t] * scale * gain_ref[:, cols]).astype(jnp.bfloat16)

    def turn(values, factor):
        wide = values.astype(jnp.bfloat16).astype(jnp.float32)
        swapped = jnp.where(
            is_first, pltpu.roll(wide, 128 - half, 1), pltpu.roll(wide, half, 1)
        )
        return ((wide * cos_ref[...] + swapped * sin_ref[...]) * factor).astype(jnp.bfloat16)

    def project(g):
        return jnp.dot(normed[...], wg[g], preferred_element_type=jnp.float32)

    mid = pl.ds(WINDOW, rows)
    edge = 16
    has_next, has_prev = block_of + 1 < nsp, block_of >= 1
    next_at = at(z + c, y, x, 1 - c)
    prev_at = at(z + c - 1, y, x, 1 - c)

    def halo_copy(way, what):
        cols = pl.ds(0, gw) if what == 0 else pl.ds(gw, pn)
        count = WINDOW if what == 0 else edge
        if way == 0:
            src, dst = WINDOW + rows - count, WINDOW - count
        else:
            src, dst = WINDOW, WINDOW + rows
        return remote(
            ext.at[pl.ds(src, count), cols],
            ext.at[pl.ds(dst, count), cols],
            h_send.at[way, what],
            h_recv.at[way, what],
            next_at if way == 0 else prev_at,
        )

    def halo_send(what, done=False):
        for way, ok in ((0, has_next), (1, has_prev)):

            @pl.when(ok)
            def _():
                issue(halo_copy(way, what), done)

    def halo_wait(what, near):
        for way, ok in ((0, has_prev), (1, has_next)):
            inside_chip = c == 1 if way == 0 else c == 0

            @pl.when(ok & (inside_chip if near else jnp.logical_not(inside_chip)))
            def _():
                halo_copy(way, what).wait_recv()

    gathered(0)
    pair = project(0)
    for col in range(0, kn, 128):
        ext[mid, col : col + 128] = turn(pair[:, col : col + 128], 1.0)
    ext[mid, kn:gw] = pair[:, kn:].astype(jnp.bfloat16)
    halo_send(0)

    stage(nz, nz + 1)
    for p in range(groups, pieces):
        load_wait(p)
        send_own(p, (2,))
        for way in range(2):

            @pl.when(onward[way] & (behind[way] <= 1))
            def _():
                w_copy(p, block_of, way).start()

    span = 3 * WINDOW
    row_at = lax.broadcasted_iota(jnp.int32, (WINDOW, span), 0)
    key_at = lax.broadcasted_iota(jnp.int32, (WINDOW, span), 1)
    apart = key_at - row_at
    lane_at = lax.broadcasted_iota(jnp.int32, (WINDOW, 128), 1)
    half_width = jnp.left_shift(jnp.int32(1), group_of)
    n_blocks = rows // WINDOW

    def inside_of(i):
        first = block_of * rows + (i - 1) * WINDOW
        return (key_at + first >= 0) & (key_at + first < seq_total)

    def attend(kv, i):
        q_at = pl.ds(pl.multiple_of(i * WINDOW, WINDOW), WINDOW)
        window = pl.ds(pl.multiple_of(i * WINDOW, WINDOW), span)
        valid = inside_of(i) & (apart >= 0) & (apart <= 2 * WINDOW)
        logs = jnp.zeros((WINDOW, 128), jnp.float32)
        keys = ext[window, kv * HD : (kv + 1) * HD]
        values = ext[window, kn + kv * HD : kn + (kv + 1) * HD]
        outs = []
        for g in range(grp):
            head = kv * grp + g
            query = qrot[q_at, head * HD : (head + 1) * HD]
            score = lax.dot_general(
                query, keys, (((1,), (1,)), ((), ())), preferred_element_type=jnp.float32
            )
            score = jnp.where(valid, score, neg_fill)
            sink = sinkb[head : head + 1, 0:1]
            top = jnp.maximum(jnp.max(score, -1, keepdims=True), sink)
            exps = jnp.exp(score - top)
            total = jnp.sum(exps, -1, keepdims=True) + jnp.exp(sink - top)
            weights = (exps * (1.0 / total)).astype(jnp.bfloat16)
            outs.append(jnp.dot(weights, values, preferred_element_type=jnp.float32))
            logs = jnp.where(lane_at == g, top + jnp.log(total), logs)
        for g in range(0, grp, 2):
            col = pn + (kv * grp + g) * HD
            act[q_at, col : col + 2 * HD] = jnp.concatenate(outs[g : g + 2], 1).astype(
                jnp.bfloat16
            )
        log_own[kv * grp : (kv + 1) * grp, q_at] = logs.T[:grp, :]

    late = jnp.where(c == 0, 0, n_blocks - 1)
    early = n_blocks - 1 - late

    def attend_early(kv):
        @pl.loop(0, n_blocks - 1)
        def _(j):
            attend(kv, jnp.where(j < n_blocks - 2, j + 1, early))

    def queries(kv, g):
        both = project(g)
        for col in range(0, gw, 128):
            qrot[:, kv * gw + col : kv * gw + col + 128] = turn(
                both[:, col : col + 128], HD ** -0.5
            )

    @pl.when(crossed)
    def _():
        remote(sink_own, sinkb, m_send.at[1], m_recv.at[1], partner).wait_recv()

    gathered(1)
    queries(0, 1)
    halo_wait(0, True)
    attend_early(0)

    stage(nz + 1, nz + 2)
    gathered(2)
    ext[mid, gw : gw + pn] = project(2).astype(jnp.bfloat16)
    halo_send(1)
    for p in range(groups, pieces):
        for way in range(2):

            @pl.when(onward[way] & (behind[way] > 1))
            def _():
                w_copy(p, block_of, way).start()

    stage(nz + 2, nz + groups)
    gathered(3)
    queries(1, 3)
    attend_early(1)

    if nz > 1:
        for p in range(groups, pieces):
            relay(1, p)

    halo_wait(0, False)
    for kv in range(kv_local):
        attend(kv, late)
    log_swap = remote(log_own, log_in, m_send.at[2], m_recv.at[2], partner)

    @pl.when(crossed)
    def _():
        log_swap.start()

    for near in (True, False):
        halo_wait(1, near)

    @pl.when(straight)
    def _():
        mix_local.wait()

    @pl.when(crossed)
    def _():
        mix_swap.wait_recv()

    @pl.loop(0, n_blocks)
    def _(i):
        q_at = pl.ds(pl.multiple_of(i * WINDOW, WINDOW), WINDOW)
        window = pl.ds(pl.multiple_of(i * WINDOW, WINDOW), span)
        own_at = pl.ds(pl.multiple_of((i + 1) * WINDOW, WINDOW), WINDOW)
        band = inside_of(i) & (apart >= WINDOW - half_width) & (apart < WINDOW + half_width)
        band_f = band.astype(jnp.float32)
        counted = jnp.sum(band_f, -1, keepdims=True)
        summed = jnp.dot(
            band_f.astype(jnp.bfloat16),
            ext[window, gw : gw + pn],
            preferred_element_type=jnp.float32,
        )
        own_pool = ext[own_at, gw : gw + pn]
        pooled = (summed / counted - own_pool.astype(jnp.float32)).astype(jnp.bfloat16)
        act[q_at, 0:pn] = jnp.dot(
            pooled, mixb[...], preferred_element_type=jnp.float32
        ).astype(jnp.bfloat16)

    hrow = rows // 2

    def r1_copy(block, h, rh):
        take = pl.ds(rh * hrow, hrow)
        return remote(
            part.at[block, h, take],
            rs1.at[block, h, take],
            r1_send.at[block, h, rh],
            r1_recv.at[block, h, rh],
            at(z, 1 - y, x, c),
        )

    def r2_copy(block, h, rh):
        take = pl.ds(rh * hrow, hrow)
        owner = block // per_owner
        slot = block % per_owner
        return remote(
            tot.at[block, h, take],
            fin.at[x, slot, h, take],
            r2_send.at[block, h, rh],
            r2_recv.at[x, slot, h, rh],
            (sp, owner),
        )

    def each_block(d, body):
        @pl.loop(0, 2 if d == 0 else 4)
        def _(k):
            source = z + (2 * (k // 2) - 1) * d

            @pl.when((source >= 0) & (source < nz))
            def _():
                mine = k % 2 == 0
                body(source * NY + jnp.where(mine, c, 1 - c), mine)

    def compute(d, h):
        def body(block, mine):
            @pl.when(jnp.logical_not(mine))
            def _():
                w_copy(groups + h, block, 2).wait_recv()

            part[block, h] = jnp.dot(
                act[...], wo[block, h], preferred_element_type=jnp.float32
            ).astype(jnp.bfloat16)

            @pl.when(crossed)
            def _():
                for rh in range(2):
                    r1_copy(block, h, rh).start()

        each_block(d, body)

    def join(d, h):
        def body(block, mine):
            for rh in range(2):
                take = pl.ds(rh * hrow, hrow)
                r1_copy(block, h, rh).wait_recv()
                tot[block, h, take] = (
                    part[block, h, take].astype(jnp.float32)
                    + rs1[block, h, take].astype(jnp.float32)
                ).astype(jnp.bfloat16)

                @pl.when(block // per_owner != tp)
                def _():
                    r2_copy(block, h, rh).start()

        @pl.when(straight)
        def _():
            each_block(d, body)

    order = [(d, h) for d in range(nz) for h in range(HALVES)]
    for n, (d, h) in enumerate(order):
        if d >= 2:
            relay(d, groups + h)
        compute(d, h)
        if n >= 1:
            join(*order[n - 1])
    join(*order[-1])

    @pl.when(straight)
    def _():
        log_ref[...] = log_own[...]

    @pl.when(crossed)
    def _():
        log_swap.wait_recv()
        log_ref[...] = log_in[...]

    for slot in range(per_owner):
        block = tp * per_owner + slot
        for h in range(HALVES):
            for rh in range(2):
                take = pl.ds(rh * hrow, hrow)
                for ok, side in ((crossed, x), (x >= 0, 1 - x)):

                    @pl.when(ok)
                    def _():
                        ref = fin.at[side, slot, h, take]
                        remote(
                            ref, ref, r2_send.at[0, h, rh], r2_recv.at[side, slot, h, rh], sibling
                        ).wait_recv()

                cols = slice(slot * HALVES * ohalf + h * ohalf, slot * HALVES * ohalf + (h + 1) * ohalf)
                far = fin[1 - x, slot, h, take].astype(jnp.float32)

                @pl.when(straight)
                def _():
                    near = tot[block, h, take].astype(jnp.float32)
                    mixed_ref[take, cols] = (near + far).astype(jnp.bfloat16)

                @pl.when(crossed)
                def _():
                    near = fin[x, slot, h, take].astype(jnp.float32)
                    mixed_ref[take, cols] = (near + far).astype(jnp.bfloat16)

    for p in range(pieces):
        send_own(p, (0, 1, 2), done=True)
        for d in range(1, nz):
            relay(d, p, done=True)
    halo_send(0, done=True)
    halo_send(1, done=True)

    for r, ok in ((0, straight), (1, crossed)):

        @pl.when(ok)
        def _():
            for kind in range(3):
                if not (r == 0 and kind == 0):
                    for s in range(2):
                        token_copy(kind, s).wait_send()
            for k in range(CORES):
                token_relay(k, r).wait_send()

    @pl.when(crossed)
    def _():
        for p in range(pieces):
            for copy in load_swap(p):
                copy.wait_send()
        mix_swap.wait_send()
        sink_swap.wait_send()
        log_swap.wait_send()

    @pl.loop(0, nsp)
    def _(block):
        for h in range(HALVES):
            for rh in range(2):

                @pl.when(crossed)
                def _():
                    r1_copy(block, h, rh).wait_send()

                @pl.when(straight & (block // per_owner != tp))
                def _():
                    r2_copy(block, h, rh).wait_send()


def fused(
    nz,
    ntp,
    tokens,
    norm_gain,
    query_weight,
    key_weight,
    value_weight,
    pool_in_weight,
    pool_mix_weight,
    sink_logit,
    out_pool_weight,
    out_attn_weight,
):
    rows, width = tokens.shape
    nsp = nz * NY
    dim = width * ntp
    qn, kn, pn = query_weight.shape[1], key_weight.shape[1], pool_in_weight.shape[1]
    fan = out_pool_weight.shape[0] + out_attn_weight.shape[0]
    ohalf = out_pool_weight.shape[1] // HALVES
    heads = sink_logit.shape[0]
    gw = 2 * kn
    groups = (qn + 2 * kn + pn) // gw
    pieces = groups + HALVES
    hbm = pl.BlockSpec(memory_space=pl.ANY)
    vmem = pl.BlockSpec(memory_space=pltpu.VMEM)
    smem = pl.BlockSpec(memory_space=pltpu.SMEM)
    dma = pltpu.SemaphoreType.DMA
    bf16 = jnp.bfloat16
    f32 = jnp.float32
    per_owner = nsp // ntp
    return pl.pallas_call(
        functools.partial(layer_kernel, nz, ntp),
        out_shape=(
            jax.ShapeDtypeStruct((rows, width), bf16),
            jax.ShapeDtypeStruct((heads, rows), f32),
        ),
        in_specs=[hbm, vmem, hbm, hbm, hbm, hbm, hbm, smem, hbm, hbm],
        out_specs=(vmem, vmem),
        scratch_shapes=[
            pltpu.VMEM((ntp, rows, width), bf16),
            pltpu.VMEM((rows, dim), bf16),
            pltpu.VMEM((groups, dim, gw), bf16),
            pltpu.VMEM((nsp, HALVES, fan, ohalf), bf16),
            pltpu.VMEM((rows, qn), bf16),
            pltpu.VMEM((rows + 2 * WINDOW, gw + pn), bf16),
            pltpu.VMEM((rows, fan), bf16),
            pltpu.VMEM((nsp, HALVES, rows, ohalf), bf16),
            pltpu.VMEM((nsp, HALVES, rows, ohalf), bf16),
            pltpu.VMEM((nsp, HALVES, rows, ohalf), bf16),
            pltpu.VMEM((NX, per_owner, HALVES, rows, ohalf), bf16),
            pltpu.VMEM((rows, 128), f32),
            pltpu.VMEM((rows, 128), f32),
            pltpu.VMEM((pn, pn), bf16),
            pltpu.VMEM((heads, 128), f32),
            pltpu.VMEM((heads, 128), f32),
            pltpu.VMEM((heads, rows), f32),
            pltpu.VMEM((heads, rows), f32),
            dma((pieces, 2)),
            dma((pieces, 2)),
            dma((3, pieces, nsp)),
            dma((pieces, nsp)),
            dma,
            dma((3, 2)),
            dma((ntp, 2)),
            dma((CORES,)),
            dma((3,)),
            dma((3,)),
            dma((2, 2)),
            dma((2, 2)),
            dma((nsp, HALVES, 2)),
            dma((nsp, HALVES, 2)),
            dma((nsp, HALVES, 2)),
            dma((NX, per_owner, HALVES, 2)),
        ],
        compiler_params=pltpu.CompilerParams(
            collective_id=0, has_side_effects=True, vmem_limit_bytes=56 << 20
        ),
    )(
        tokens,
        norm_gain[None, :],
        query_weight,
        key_weight,
        value_weight,
        pool_in_weight,
        pool_mix_weight,
        sink_logit,
        out_pool_weight,
        out_attn_weight,
    )


def choose(mesh):
    nsp, ntp = mesh.shape["sp"], mesh.shape["tp"]

    def body(*args):
        rows = args[0].shape[0]
        qn, kn, pn = args[2].shape[1], args[3].shape[1], args[5].shape[1]
        columns = args[8].shape[1]
        grid = nsp % NY == 0 and ntp == NX * CORES and nsp % ntp == 0
        cuts = columns % (HALVES * 128) == 0 and rows % (4 * WINDOW) == 0
        even = kn == 2 * HD and kn % 128 == 0 and qn == 4 * kn and pn == 2 * kn
        if grid and cuts and even:
            return fused(nsp // NY, ntp, *args)
        return local(*args)

    return body


def solution(mesh):
    return jax.shard_map(
        choose(mesh),
        mesh=mesh,
        in_specs=(
            P("sp", "tp"),
            P(),
            P("sp", "tp"),
            P("sp", "tp"),
            P("sp", "tp"),
            P("sp", "tp"),
            P("tp", None, None),
            P("tp"),
            P("tp", "sp"),
            P("tp", "sp"),
        ),
        out_specs=(P("sp", "tp"), P("tp", "sp")),
        check_vma=False,
    )
```

```python
import functools
import math

import jax
import jax.numpy as jnp
from jax import lax
from jax.experimental import pallas as pl
from jax.experimental.pallas import tpu as pltpu
from jax.sharding import PartitionSpec as P

HD = 64
WINDOW = 128
GRID_W = 64


norm_eps = 1e-06
rope_base = 10000.0
pool_reach = 8
neg_fill = -1e30


def with_halo(cells, sides, width):
    for axis, dim in sides:
        count = lax.axis_size(axis)
        ends = count - 1
        head = lax.slice_in_dim(cells, 0, width, axis=dim)
        tail = lax.slice_in_dim(cells, cells.shape[dim] - width, cells.shape[dim], axis=dim)
        cells = jnp.concatenate(
            [
                lax.ppermute(tail, axis, [(i, (i + 1) % count) for i in range(ends)]),
                cells,
                lax.ppermute(head, axis, [((i + 1) % count, i) for i in range(ends)]),
            ],
            axis=dim,
        )
    return cells


def rope_tables(positions, head_dim):
    n_freq = head_dim // 4
    freqs = rope_base ** (-jnp.arange(n_freq, dtype=jnp.float32) / n_freq)
    rows = (positions // GRID_W).astype(jnp.float32)
    columns = (positions % GRID_W).astype(jnp.float32)
    row_angle = rows[:, None] * freqs[None, :]
    col_angle = columns[:, None] * freqs[None, :]
    return (jnp.cos(row_angle), jnp.sin(row_angle), jnp.cos(col_angle), jnp.sin(col_angle))


def rotate_half(values, cosine, sine):
    middle = values.shape[-1] // 2
    first = values[..., :middle]
    second = values[..., middle:]
    return jnp.concatenate([first * cosine - second * sine, second * cosine + first * sine], -1)


def rotate_heads(values, tables, head_dim):
    rows_count = values.shape[0]
    shaped = values.astype(jnp.float32).reshape(rows_count, -1, head_dim)
    cos_r, sin_r, cos_c, sin_c = [table[:, None, :] for table in tables]
    split = head_dim // 2
    turned = jnp.concatenate(
        [
            rotate_half(shaped[..., :split], cos_r, sin_r),
            rotate_half(shaped[..., split:], cos_c, sin_c),
        ],
        -1,
    )
    return turned.reshape(rows_count, -1).astype(jnp.bfloat16)


def pool_group(extended, own, positions, half_width, seq_total):
    rows_count = own.shape[0]
    summed = jnp.zeros(own.shape, jnp.float32)
    counted = jnp.zeros((rows_count,), jnp.float32)
    for shift_by in range(-pool_reach, pool_reach):
        source = positions + shift_by
        inside = (
            (shift_by >= -half_width)
            & (shift_by < half_width)
            & (source >= 0)
            & (source < seq_total)
        )
        window_rows = extended[pool_reach + shift_by : pool_reach + shift_by + rows_count].astype(
            jnp.float32
        )
        summed = summed + jnp.where(inside[:, None], window_rows, 0.0)
        counted = counted + inside.astype(jnp.float32)
    return (summed / counted[:, None] - own.astype(jnp.float32)).astype(jnp.bfloat16)


def attend_block(queries, keys, values, sink, query_pos, key_pos, seq_total):
    scores = jnp.einsum(
        "qhgd,khd->hgqk", queries, keys, preferred_element_type=jnp.float32
    ) * HD ** (-0.5)
    valid = (
        (jnp.abs(query_pos[:, None] - key_pos[None, :]) <= WINDOW)
        & (key_pos >= 0)[None, :]
        & (key_pos < seq_total)[None, :]
    )
    scores = jnp.where(valid, scores, neg_fill)
    row_top = jnp.maximum(jnp.max(scores, -1), sink[:, :, None])
    exps = jnp.exp(scores - row_top[..., None])
    row_total = jnp.sum(exps, -1) + jnp.exp(sink[:, :, None] - row_top)
    weights = (exps / row_total[..., None]).astype(jnp.bfloat16)
    attended = jnp.einsum("hgqk,khd->qhgd", weights, values, preferred_element_type=jnp.float32)
    return (attended.astype(jnp.bfloat16), row_top + jnp.log(row_total))


def fetch_outputs(out_pool_weight, out_attn_weight):
    return (
        lax.all_gather(out_pool_weight, "sp", axis=1, tiled=True),
        lax.all_gather(out_attn_weight, "sp", axis=1, tiled=True),
    )


def local(
    tokens,
    norm_gain,
    query_weight,
    key_weight,
    value_weight,
    pool_in_weight,
    pool_mix_weight,
    sink_logit,
    out_pool_weight,
    out_attn_weight,
):
    whole = lax.all_gather(tokens, "tp", axis=1, tiled=True)
    wide = whole.astype(jnp.float32)
    normed = (
        wide * lax.rsqrt(jnp.mean(wide * wide, -1, keepdims=True) + norm_eps) * norm_gain
    ).astype(jnp.bfloat16)
    tok_rows = normed.shape[0]
    seq_total = tok_rows * lax.axis_size("sp")
    offset = lax.axis_index("sp") * tok_rows
    weights_in = (query_weight, key_weight, value_weight, pool_in_weight)
    pieces = (
        lax.all_gather(weights_in[0], "sp", axis=0, tiled=True),
        lax.all_gather(weights_in[1], "sp", axis=0, tiled=True),
        lax.all_gather(weights_in[2], "sp", axis=0, tiled=True),
        lax.all_gather(weights_in[3], "sp", axis=0, tiled=True),
    )
    sums = tuple((jnp.dot(normed, piece, preferred_element_type=jnp.float32) for piece in pieces))
    query, key, value, pool_input = [total.astype(jnp.bfloat16) for total in sums]
    positions = offset + jnp.arange(tok_rows, dtype=jnp.int32)
    tables = rope_tables(positions, HD)
    rot_query = rotate_heads(query, tables, HD)
    rot_key = rotate_heads(key, tables, HD)
    key_width = rot_key.shape[1]
    pool_ext = with_halo(pool_input, (("sp", 0),), pool_reach)
    pair_ext = with_halo(jnp.concatenate([rot_key, value], 1), (("sp", 0),), WINDOW)
    key_ext = pair_ext[:, :key_width]
    value_ext = pair_ext[:, key_width:]
    half_width = jnp.left_shift(jnp.int32(1), lax.axis_index("tp"))
    pooled = pool_group(pool_ext, pool_input, positions, half_width, seq_total)
    pool_out = jnp.dot(pooled, pool_mix_weight[0], preferred_element_type=jnp.float32).astype(
        jnp.bfloat16
    )
    heads_local = rot_query.shape[1] // HD
    kv_local = key_width // HD
    grp = heads_local // kv_local
    query_heads = rot_query.reshape(tok_rows, kv_local, grp, HD)
    key_heads = key_ext.reshape(-1, kv_local, HD)
    value_heads = value_ext.reshape(-1, kv_local, HD)
    sink = sink_logit.reshape(kv_local, grp)
    block_rows = min(tok_rows, 256)
    attended_parts = []
    log_parts = []
    for block_index in range(tok_rows // block_rows):
        start = block_index * block_rows
        query_pos = offset + start + jnp.arange(block_rows, dtype=jnp.int32)
        key_pos = offset + start - WINDOW + jnp.arange(block_rows + 2 * WINDOW, dtype=jnp.int32)
        attended_block, log_block = attend_block(
            query_heads[start : start + block_rows],
            key_heads[start : start + block_rows + 2 * WINDOW],
            value_heads[start : start + block_rows + 2 * WINDOW],
            sink,
            query_pos,
            key_pos,
            seq_total,
        )
        attended_parts.append(attended_block.reshape(block_rows, heads_local * HD))
        log_parts.append(log_block.reshape(heads_local, block_rows))
    attended = jnp.concatenate(attended_parts, 0)
    log_weight = jnp.concatenate(log_parts, 1)
    out_pool_full, out_attn_full = fetch_outputs(out_pool_weight, out_attn_weight)
    term = jnp.dot(pool_out, out_pool_full, preferred_element_type=jnp.float32)
    term = term + jnp.dot(attended, out_attn_full, preferred_element_type=jnp.float32)
    mixed = lax.psum_scatter(term.astype(jnp.bfloat16), "tp", scatter_dimension=1, tiled=True)
    return (mixed, log_weight)


NY = 2
NX = 2
CORES = 2
HALVES = 2
MESH = pl.DeviceIdType.MESH


def layer_kernel(
    nz,
    ntp,
    tok_ref,
    gain_ref,
    qw_ref,
    kw_ref,
    vw_ref,
    pw_ref,
    mix_ref,
    sink_ref,
    ow_ref,
    aw_ref,
    mixed_ref,
    log_ref,
    xg,
    normed,
    wg,
    wo,
    qrot,
    ext,
    act,
    part,
    rs1,
    tot,
    fin,
    cos_ref,
    sin_ref,
    mixb,
    gain,
    sinks,
    sink_own,
    sinkb,
    log_own,
    log_in,
    load_send,
    load_recv,
    w_send,
    w_recv,
    s_recv,
    o_recv,
    x_loc,
    x_send,
    x_recv,
    g_sem,
    m_send,
    m_recv,
    h_send,
    h_recv,
    r1_send,
    r1_recv,
    r2_send,
    r2_recv,
):
    sp, tp = lax.axis_index("sp"), lax.axis_index("tp")
    z, y = sp // NY, sp % NY
    x, c = tp // CORES, tp % CORES
    nsp = nz * NY
    block_of = z * NY + c
    group_of = x * CORES + y
    straight = c == y
    crossed = c != y
    rows, width = tok_ref.shape
    brow = qw_ref.shape[0]
    qn, kn, pn = qw_ref.shape[1], kw_ref.shape[1], pw_ref.shape[1]
    heads, kv_local = qn // HD, kn // HD
    grp = heads // kv_local
    gw = 2 * kn
    groups = wg.shape[0]
    pool_rows = ow_ref.shape[0]
    ohalf = wo.shape[3]
    seq_total = rows * nsp
    per_owner = nsp // ntp
    pieces = groups + HALVES

    def at(zz, yy, xx, cc):
        return (zz * NY + yy, xx * CORES + cc)

    def remote(src, dst, send, recv, target):
        return pltpu.make_async_remote_copy(
            src_ref=src,
            dst_ref=dst,
            send_sem=send,
            recv_sem=recv,
            device_id=target,
            device_id_type=MESH,
        )

    sibling = at(z, y, x, 1 - c)
    partner = at(z, 1 - y, x, 1 - c)

    def shard_rows(block):
        return pl.ds(pl.multiple_of(block * brow, brow), brow)

    def load_parts(p, block):
        if p == 0:
            return [
                (kw_ref, wg.at[0, shard_rows(block), pl.ds(0, kn)]),
                (vw_ref, wg.at[0, shard_rows(block), pl.ds(kn, kn)]),
            ]
        if p == 1:
            return [(pw_ref, wg.at[1, shard_rows(block)])]
        if p < groups:
            return [(qw_ref.at[:, pl.ds((p - 2) * gw, gw)], wg.at[p, shard_rows(block)])]
        h = p - groups
        cols = pl.ds(h * ohalf, ohalf)
        return [
            (ow_ref.at[:, cols], wo.at[block, h, pl.ds(0, pool_rows)]),
            (aw_ref.at[:, cols], wo.at[block, h, pl.ds(pool_rows, wo.shape[2] - pool_rows)]),
        ]

    def load_local(p):
        return [
            pltpu.make_async_copy(a, b, load_recv.at[p]) for a, b in load_parts(p, sp)
        ]

    def load_swap(p):
        return [
            remote(a, b, load_send.at[p // groups], load_recv.at[p], partner)
            for a, b in load_parts(p, sp)
        ]

    def piece_of(p, block):
        return wg.at[p, shard_rows(block)] if p < groups else wo.at[block, p - groups]

    def arrived(ref, sem):
        remote(ref, ref, load_send.at[0], sem, sibling).wait_recv()

    def departed(ref, sem):
        remote(ref, ref, sem, load_recv.at[0], sibling).wait_send()

    def load_wait(p):
        arrived(piece_of(p, block_of), load_recv.at[p])

    onward = (z + 1 < nz, z >= 1)
    middle = onward[0] & onward[1]
    outer = jnp.logical_not(middle)

    def w_copy(p, block, way):
        ref = piece_of(p, block)
        target = (at(z + 1, y, x, c), at(z - 1, y, x, c), sibling)[way]
        if way < 2:
            recv = w_recv.at[p, block // NY]
        elif p < groups:
            recv = s_recv.at[p]
        else:
            recv = o_recv.at[p - groups, block // NY]
        return remote(ref, ref, w_send.at[way, p // groups], recv, target)

    def send_own(p, ways):
        for way in ways:
            if way == 2:
                w_copy(p, block_of, 2).start()
            else:

                @pl.when(onward[way])
                def _():
                    w_copy(p, block_of, way).start()

    def relay(d, p):
        for way in range(2):
            source = (z - d, z + d)[way]
            block = source * NY + c

            @pl.when((source >= 0) & (source < nz))
            def _():
                w_copy(p, block, way).wait_recv()

                @pl.when(onward[way])
                def _():
                    w_copy(p, block, way).start()

                w_copy(p, block, 2).start()

    def stage(low, high, ok=None):
        if ok is not None:

            @pl.when(ok)
            def _():
                stage(low, high)

            return
        for turn_at in range(low, high):
            for p in range(groups):
                for role, when in ((straight, max(p - 1, 0)), (crossed, max(2 * p - 1, 0))):
                    if when == turn_at:

                        @pl.when(role)
                        def _():
                            load_wait(p)
                            send_own(p, (0, 1, 2))

            for d in range(1, nz):
                for p in range(groups):
                    if turn_at == 2 * p + d:
                        relay(d, p)

    def gathered(p):
        arrived(wg.at[p, pl.ds(0, nz * brow)], s_recv.at[p])

    cut = rows // 4
    spans = (pl.ds(0, cut), pl.ds(cut, rows - cut))

    def token_copy(kind, r):
        target = (at(z, y, x, y), at(z, y, 1 - x, y), at(z, 1 - y, x, y))[kind]
        return remote(
            tok_ref.at[spans[r]], xg.at[tp, spans[r]], x_send.at[0], x_recv.at[tp, r], target
        )

    token_local = pltpu.make_async_copy(tok_ref, xg.at[tp], x_loc)

    def token_relay(k, r):
        slot = ((1 - x) if r == 0 else x) * CORES + k
        target = at(z, 1 - y, x, c) if r == 0 else at(z, y, 1 - x, c)
        ref = xg.at[slot, spans[r]]
        return remote(ref, ref, x_send.at[1], x_recv.at[slot, r], target)

    def token_wait(slot, r):
        arrived(xg.at[slot, spans[r]], x_recv.at[slot, r])

    mix_local = pltpu.make_async_copy(mix_ref.at[0], mixb, m_recv.at[0])
    mix_swap = remote(mix_ref.at[0], mixb, m_send.at[0], m_recv.at[0], partner)
    sink_swap = remote(sink_own, sinkb, m_send.at[1], m_recv.at[1], partner)

    gain_load = pltpu.make_async_copy(gain_ref, gain, g_sem.at[0])
    sink_load = pltpu.make_async_copy(sink_ref, sinks, g_sem.at[1])
    sink_load.start()
    gain_load.start()

    @pl.when(straight)
    def _():
        for p in range(groups):
            for copy in load_local(p):
                copy.start()
        token_local.start()

    barrier = pltpu.get_barrier_semaphore()
    met = jnp.int32(0)
    for flip in range(1, NY * NX * CORES):
        fy, fx, fc = flip // 4, (flip // 2) % 2, flip % 2
        pl.semaphore_signal(
            barrier,
            inc=1,
            device_id=at(
                z,
                1 - y if fy else y,
                1 - x if fx else x,
                1 - c if fc else c,
            ),
            device_id_type=MESH,
        )
        met = met + 1
    for ok, zz in ((onward[0], z + 1), (onward[1], z - 1)):
        met = met + CORES * ok.astype(jnp.int32)

        @pl.when(ok)
        def _():
            for cc in range(CORES):
                pl.semaphore_signal(
                    barrier, inc=1, device_id=at(zz, y, x, cc), device_id_type=MESH
                )

    ext[...] = jnp.zeros_like(ext)
    sink_load.wait()
    for head in range(heads):
        sink_own[head : head + 1, :] = jnp.full((1, 128), sinks[head], jnp.float32)

    @pl.when(straight)
    def _():
        sinkb[...] = sink_own[...]

    pl.semaphore_wait(barrier, met)

    @pl.when(straight)
    def _():
        for kind in (1, 2):
            for r in range(2):
                token_copy(kind, r if kind == 1 else 1 - r).start()
        mix_local.start()
        for p in range(groups, pieces):
            for copy in load_local(p):
                copy.start()

    @pl.when(crossed)
    def _():
        for r in range(2):
            token_copy(1, r).start()
            token_copy(0, r).start()
        for p in range(groups):
            if p == 2:
                token_copy(2, 1).start()
            for copy in load_swap(p):
                copy.start()
        token_copy(2, 0).start()
        sink_swap.start()
        mix_swap.start()
        for p in range(groups, pieces):
            for copy in load_swap(p):
                copy.start()

    stage(0, 1)

    half = HD // 4
    lane = lax.broadcasted_iota(jnp.int32, (rows, 128), 1)
    is_first = (lane % (2 * half)) < half
    position = block_of * rows + lax.broadcasted_iota(jnp.int32, (rows, 128), 0)
    place = jnp.where((lane % HD) < 2 * half, position // GRID_W, position % GRID_W)
    freqs = jnp.exp((lane % half).astype(jnp.float32) * (-math.log(rope_base) / half))
    angle = place.astype(jnp.float32) * freqs
    cos_ref[...] = jnp.cos(angle)
    sine = jnp.sin(angle)
    sin_ref[...] = jnp.where(is_first, -sine, sine)

    stage(1, 2)

    @pl.when(straight)
    def _():
        for k in range(CORES):
            token_relay(k, 0).wait_recv()
            token_relay(k, 0).start()

    @pl.when(crossed)
    def _():
        token_relay(c, 1).wait_recv()
        token_relay(c, 1).start()

    stage(2, 3)

    @pl.when(crossed)
    def _():
        token_relay(1 - c, 1).wait_recv()
        token_relay(1 - c, 1).start()

    stage(3, nz)
    stage(nz, nz + 2, middle)

    @pl.when(straight)
    def _():
        token_local.wait()
        for r in range(2):
            token_wait(x * CORES + (1 - c), r)
        for k in range(CORES):
            token_wait((1 - x) * CORES + k, 1)

    @pl.when(crossed)
    def _():
        for k in range(CORES):
            token_wait(x * CORES + k, 0)
            for r in range(2):
                token_wait((1 - x) * CORES + k, r)

    gain_load.wait()
    norm_rows = 64

    @pl.loop(0, rows // norm_rows)
    def _(i):
        take = pl.ds(pl.multiple_of(i * norm_rows, norm_rows), norm_rows)
        pieces_in = [xg[t, take, :].astype(jnp.float32) for t in range(ntp)]
        total = sum(jnp.sum(piece * piece, -1, keepdims=True) for piece in pieces_in)
        scale = lax.rsqrt(total / (width * ntp) + norm_eps)
        for t in range(ntp):
            cols = pl.ds(t * width, width)
            normed[take, cols] = (pieces_in[t] * scale * gain[:, cols]).astype(jnp.bfloat16)

    hrow = rows // 2
    lane_first = (lax.broadcasted_iota(jnp.int32, (hrow, 128), 1) % (2 * half)) < half

    def turn(values, low, factor):
        wide = values.astype(jnp.bfloat16).astype(jnp.float32)
        swapped = jnp.where(
            lane_first, pltpu.roll(wide, 128 - half, 1), pltpu.roll(wide, half, 1)
        )
        take = pl.ds(low, hrow)
        return ((wide * cos_ref[take] + swapped * sin_ref[take]) * factor).astype(jnp.bfloat16)

    def project(g, low):
        return jnp.dot(normed[pl.ds(low, hrow)], wg[g], preferred_element_type=jnp.float32)

    edge = 16
    has_next, has_prev = block_of + 1 < nsp, block_of >= 1
    next_at = at(z + c, y, x, 1 - c)
    prev_at = at(z + c - 1, y, x, 1 - c)

    def halo_copy(way, what):
        cols = pl.ds(0, gw) if what == 0 else pl.ds(gw, pn)
        count = WINDOW if what == 0 else edge
        if way == 0:
            src, dst = WINDOW + rows - count, WINDOW - count
        else:
            src, dst = WINDOW, WINDOW + rows
        return remote(
            ext.at[pl.ds(src, count), cols],
            ext.at[pl.ds(dst, count), cols],
            h_send.at[way, what],
            h_recv.at[way, what],
            next_at if way == 0 else prev_at,
        )

    def halo_send(what, done=False):
        for way, ok in ((0, has_next), (1, has_prev)):

            @pl.when(ok)
            def _():
                if done:
                    halo_copy(way, what).wait_send()
                else:
                    halo_copy(way, what).start()

    def halo_wait(what, near):
        for way, ok in ((0, has_prev), (1, has_next)):
            inside_chip = c == 1 if way == 0 else c == 0

            @pl.when(ok & (inside_chip if near else jnp.logical_not(inside_chip)))
            def _():
                halo_copy(way, what).wait_recv()

    gathered(0)
    for low in range(0, rows, hrow):
        pair = project(0, low)
        into = pl.ds(WINDOW + low, hrow)
        for col in range(0, kn, 128):
            ext[into, col : col + 128] = turn(pair[:, col : col + 128], low, 1.0)
        ext[into, kn:gw] = pair[:, kn:].astype(jnp.bfloat16)
    halo_send(0)

    stage(nz + 2, nz + 4, middle)
    stage(nz, nz + 2, outer)
    gathered(1)
    for low in range(0, rows, hrow):
        ext[pl.ds(WINDOW + low, hrow), gw : gw + pn] = project(1, low).astype(jnp.bfloat16)
    halo_send(1)
    stage(nz + 4, nz + 2 * groups, middle)
    for p in range(groups, pieces):
        load_wait(p)
        send_own(p, (0, 1, 2))

    span = 3 * WINDOW
    row_at = lax.broadcasted_iota(jnp.int32, (WINDOW, span), 0)
    key_at = lax.broadcasted_iota(jnp.int32, (WINDOW, span), 1)
    apart = key_at - row_at
    key_down = lax.broadcasted_iota(jnp.int32, (WINDOW, WINDOW), 0)
    query_over = lax.broadcasted_iota(jnp.int32, (WINDOW, WINDOW), 1)
    half_width = jnp.left_shift(jnp.int32(1), group_of)
    n_blocks = rows // WINDOW

    def inside_of(i):
        first = block_of * rows + (i - 1) * WINDOW
        return (key_at + first >= 0) & (key_at + first < seq_total)

    def attend(kv, i):
        q_at = pl.ds(pl.multiple_of(i * WINDOW, WINDOW), WINDOW)
        window = pl.ds(pl.multiple_of(i * WINDOW, WINDOW), span)
        first = block_of * rows + (i - 1) * WINDOW
        low = (key_down >= query_over) & (first >= 0)
        high = (key_down <= query_over) & (first + 2 * WINDOW < seq_total)
        keys = ext[window, kv * HD : (kv + 1) * HD]
        values = ext[window, kn + kv * HD : kn + (kv + 1) * HD].T
        weights, shares = [], []
        for g in range(grp):
            head = kv * grp + g
            query = qrot[q_at, head * HD : (head + 1) * HD]
            score = lax.dot_general(
                keys, query, (((1,), (1,)), ((), ())), preferred_element_type=jnp.float32
            )
            score = jnp.concatenate(
                [
                    jnp.where(low, score[:WINDOW], neg_fill),
                    score[WINDOW : 2 * WINDOW],
                    jnp.where(high, score[2 * WINDOW :], neg_fill),
                ],
                0,
            )
            sink = sinkb[head : head + 1, :]
            top = jnp.maximum(jnp.max(score, 0, keepdims=True), sink)
            exps = jnp.exp(score - top)
            total = jnp.sum(exps, 0, keepdims=True) + jnp.exp(sink - top)
            log_own[head : head + 1, q_at] = top + jnp.log(total)
            weights.append(exps.astype(jnp.bfloat16))
            shares.append(1.0 / total)
        out = jnp.dot(values, jnp.concatenate(weights, 1), preferred_element_type=jnp.float32)
        outs = [out[:, g * WINDOW : (g + 1) * WINDOW] * shares[g] for g in range(grp)]
        col = pn + kv * grp * HD
        act[q_at, col : col + grp * HD] = jnp.concatenate(outs, 0).T.astype(jnp.bfloat16)

    late = jnp.where(c == 0, 0, n_blocks - 1)
    early = n_blocks - 1 - late

    def attend_early(kv):
        for i in range(1, n_blocks - 1):
            attend(kv, i)
        attend(kv, early)

    def queries(kv, g):
        for low in range(0, rows, hrow):
            both = project(g, low)
            for col in range(0, gw, 128):
                at_col = kv * gw + col
                qrot[pl.ds(low, hrow), at_col : at_col + 128] = turn(
                    both[:, col : col + 128], low, HD ** -0.5
                )

    @pl.when(crossed)
    def _():
        remote(sink_own, sinkb, m_send.at[1], m_recv.at[1], partner).wait_recv()

    def pool(i):
        q_at = pl.ds(pl.multiple_of(i * WINDOW, WINDOW), WINDOW)
        window = pl.ds(pl.multiple_of(i * WINDOW, WINDOW), span)
        own_at = pl.ds(pl.multiple_of((i + 1) * WINDOW, WINDOW), WINDOW)
        band = inside_of(i) & (apart >= WINDOW - half_width) & (apart < WINDOW + half_width)
        band_f = band.astype(jnp.float32)
        counted = jnp.sum(band_f, -1, keepdims=True)
        summed = jnp.dot(
            band_f.astype(jnp.bfloat16),
            ext[window, gw : gw + pn],
            preferred_element_type=jnp.float32,
        )
        own_pool = ext[own_at, gw : gw + pn]
        pooled = (summed / counted - own_pool.astype(jnp.float32)).astype(jnp.bfloat16)
        act[q_at, 0:pn] = jnp.dot(
            pooled, mixb[...], preferred_element_type=jnp.float32
        ).astype(jnp.bfloat16)

    halo_wait(1, True)

    @pl.when(straight)
    def _():
        mix_local.wait()

    @pl.when(crossed)
    def _():
        mix_swap.wait_recv()

    for i in range(1, n_blocks - 1):
        pool(i)
    pool(early)

    stage(nz + 2, nz + 4, outer)
    gathered(2)
    queries(0, 2)
    halo_wait(0, True)
    attend_early(0)
    stage(nz + 4, nz + 2 * groups, outer)
    halo_wait(0, False)
    attend(0, late)
    halo_wait(1, False)
    pool(late)

    gathered(3)
    queries(1, 3)
    attend_early(1)
    attend(1, late)
    log_swap = remote(log_own, log_in, m_send.at[2], m_recv.at[2], partner)

    @pl.when(crossed)
    def _():
        log_swap.start()

    def r1_copy(block, h, rh):
        take = pl.ds(rh * hrow, hrow)
        return remote(
            part.at[h, block, take],
            rs1.at[h, block, take],
            r1_send.at[h],
            r1_recv.at[h, block, rh],
            at(z, 1 - y, x, c),
        )

    def r2_copy(block, h, rh):
        take = pl.ds(rh * hrow, hrow)
        owner = block // per_owner
        slot = block % per_owner
        side = jnp.where(owner // CORES == x, 0, 1)
        return remote(
            tot.at[h, block, take],
            fin.at[side, h, slot, take],
            r2_send.at[h],
            r2_recv.at[side, h, slot, rh],
            (sp, owner),
        )

    def each_block(d, body):
        @pl.loop(0, 2 if d == 0 else 4)
        def _(k):
            source = z + (2 * (k // 2) - 1) * d

            @pl.when((source >= 0) & (source < nz))
            def _():
                mine = k % 2 == 0
                body(source * NY + jnp.where(mine, c, 1 - c), mine)

    def compute(d, h):
        def body(block, mine):
            @pl.when(jnp.logical_not(mine))
            def _():
                w_copy(groups + h, block, 2).wait_recv()

            part[h, block] = jnp.dot(
                act[...], wo[block, h], preferred_element_type=jnp.float32
            ).astype(jnp.bfloat16)

            @pl.when(crossed)
            def _():
                for rh in range(2):
                    r1_copy(block, h, rh).start()

        each_block(d, body)

    def join(d, h):
        def body(block, mine):
            for rh in range(2):
                take = pl.ds(rh * hrow, hrow)
                r1_copy(block, h, rh).wait_recv()
                tot[h, block, take] = (
                    part[h, block, take].astype(jnp.float32)
                    + rs1[h, block, take].astype(jnp.float32)
                ).astype(jnp.bfloat16)

                @pl.when(block // per_owner != tp)
                def _():
                    r2_copy(block, h, rh).start()

        @pl.when(straight)
        def _():
            each_block(d, body)

    def pass_on(d, h, ok):
        @pl.when(ok)
        def _():
            relay(d, groups + h)

    for h in range(HALVES):
        pass_on(1, h, middle)
    order = [(d, h) for d in range(nz) for h in range(HALVES)]
    for n, (d, h) in enumerate(order):
        if d >= 1:
            pass_on(d, h, outer)
        if d == 2:
            if h == 0:
                for far in range(2, nz):
                    for e in range(HALVES):
                        pass_on(far, e, middle)
        compute(d, h)
        if n >= 1:
            join(*order[n - 1])
    join(*order[-1])

    @pl.when(straight)
    def _():
        log_ref[...] = log_own[...]

    @pl.when(crossed)
    def _():
        log_swap.wait_recv()
        log_ref[...] = log_in[...]

    for slot in range(per_owner):
        block = tp * per_owner + slot
        for h in range(HALVES):
            low = (slot * HALVES + h) * ohalf
            for rh in range(2):
                take = pl.ds(rh * hrow, hrow)
                for ok, side in ((crossed, 0), (tp >= 0, 1)):

                    @pl.when(ok)
                    def _():
                        ref = fin.at[side, h, slot, take]
                        remote(
                            ref, ref, r2_send.at[h], r2_recv.at[side, h, slot, rh], sibling
                        ).wait_recv()

                far = fin[1, h, slot, take].astype(jnp.float32)

                @pl.when(straight)
                def _():
                    near = tot[h, block, take].astype(jnp.float32)
                    mixed_ref[take, low : low + ohalf] = (near + far).astype(jnp.bfloat16)

                @pl.when(crossed)
                def _():
                    near = fin[0, h, slot, take].astype(jnp.float32)
                    mixed_ref[take, low : low + ohalf] = (near + far).astype(jnp.bfloat16)

    def all_sent(way, count):
        departed(wg.at[pl.ds(0, groups), pl.ds(0, count * brow)], w_send.at[way, 0])
        departed(wo.at[pl.ds(0, count)], w_send.at[way, 1])

    all_sent(2, nz)
    for count in range(1, nz):
        for way, passed in ((0, z + 1), (1, nz - z)):

            @pl.when(onward[way] & (passed == count))
            def _():
                all_sent(way, count)

    halo_send(0, done=True)
    halo_send(1, done=True)

    @pl.when(straight)
    def _():
        departed(xg.at[pl.ds(0, 2)], x_send.at[0])
        departed(xg.at[pl.ds(0, CORES), spans[0]], x_send.at[1])
        for h in range(HALVES):
            departed(tot.at[h, pl.ds(0, nsp - per_owner)], r2_send.at[h])

    @pl.when(crossed)
    def _():
        departed(xg.at[pl.ds(0, 3)], x_send.at[0])
        departed(xg.at[pl.ds(0, CORES), spans[1]], x_send.at[1])
        departed(wg.at[pl.ds(0, groups), pl.ds(0, brow)], load_send.at[0])
        departed(wo.at[0], load_send.at[1])
        mix_swap.wait_send()
        sink_swap.wait_send()
        log_swap.wait_send()
        for h in range(HALVES):
            departed(part.at[h], r1_send.at[h])


def place_kernel(mixed_ref, log_ref, mixed_out, log_out, sems):
    copies = [
        pltpu.make_async_copy(mixed_ref, mixed_out, sems.at[0]),
        pltpu.make_async_copy(log_ref, log_out, sems.at[1]),
    ]
    for copy in copies:
        copy.start()
    for copy in copies:
        copy.wait()


def fused(
    nz,
    ntp,
    tokens,
    norm_gain,
    query_weight,
    key_weight,
    value_weight,
    pool_in_weight,
    pool_mix_weight,
    sink_logit,
    out_pool_weight,
    out_attn_weight,
):
    rows, width = tokens.shape
    nsp = nz * NY
    dim = width * ntp
    qn, kn, pn = query_weight.shape[1], key_weight.shape[1], pool_in_weight.shape[1]
    fan = out_pool_weight.shape[0] + out_attn_weight.shape[0]
    ohalf = out_pool_weight.shape[1] // HALVES
    heads = sink_logit.shape[0]
    gw = 2 * kn
    groups = (qn + 2 * kn + pn) // gw
    pieces = groups + HALVES
    hbm = pl.BlockSpec(memory_space=pl.ANY)
    vmem = pl.BlockSpec(memory_space=pltpu.VMEM)
    dma = pltpu.SemaphoreType.DMA
    bf16 = jnp.bfloat16
    f32 = jnp.float32
    per_owner = nsp // ntp
    outs = (
        jax.ShapeDtypeStruct((rows, width), bf16),
        jax.ShapeDtypeStruct((heads, rows), f32),
    )
    mixed, logs = pl.pallas_call(
        functools.partial(layer_kernel, nz, ntp),
        out_shape=outs,
        in_specs=[hbm] * 10,
        out_specs=(vmem, vmem),
        scratch_shapes=[
            pltpu.VMEM((ntp, rows, width), bf16),
            pltpu.VMEM((rows, dim), bf16),
            pltpu.VMEM((groups, dim, gw), bf16),
            pltpu.VMEM((nsp, HALVES, fan, ohalf), bf16),
            pltpu.VMEM((rows, qn), bf16),
            pltpu.VMEM((rows + 2 * WINDOW, gw + pn), bf16),
            pltpu.VMEM((rows, fan), bf16),
            pltpu.VMEM((HALVES, nsp, rows, ohalf), bf16),
            pltpu.VMEM((HALVES, nsp, rows, ohalf), bf16),
            pltpu.VMEM((HALVES, nsp, rows, ohalf), bf16),
            pltpu.VMEM((2, HALVES, per_owner, rows, ohalf), bf16),
            pltpu.VMEM((rows, 128), f32),
            pltpu.VMEM((rows, 128), f32),
            pltpu.VMEM((pn, pn), bf16),
            pltpu.VMEM((1, dim), f32),
            pltpu.SMEM((heads,), f32),
            pltpu.VMEM((heads, 128), f32),
            pltpu.VMEM((heads, 128), f32),
            pltpu.VMEM((heads, rows), f32),
            pltpu.VMEM((heads, rows), f32),
            dma((2,)),
            dma((pieces,)),
            dma((3, 2)),
            dma((pieces, nz)),
            dma((groups,)),
            dma((HALVES, nz)),
            dma,
            dma((2,)),
            dma((ntp, 2)),
            dma((2,)),
            dma((3,)),
            dma((3,)),
            dma((2, 2)),
            dma((2, 2)),
            dma((HALVES,)),
            dma((HALVES, nsp, 2)),
            dma((HALVES,)),
            dma((2, HALVES, per_owner, 2)),
        ],
        compiler_params=pltpu.CompilerParams(
            collective_id=0, has_side_effects=True, vmem_limit_bytes=56 << 20
        ),
    )(
        tokens,
        norm_gain[None, :],
        query_weight,
        key_weight,
        value_weight,
        pool_in_weight,
        pool_mix_weight,
        sink_logit,
        out_pool_weight,
        out_attn_weight,
    )
    return pl.pallas_call(
        place_kernel,
        out_shape=outs,
        in_specs=[vmem, vmem],
        out_specs=(hbm, hbm),
        scratch_shapes=[dma((2,))],
    )(mixed, logs)


def choose(mesh):
    nsp, ntp = mesh.shape["sp"], mesh.shape["tp"]

    def body(*args):
        rows = args[0].shape[0]
        qn, kn, pn = args[2].shape[1], args[3].shape[1], args[5].shape[1]
        columns = args[8].shape[1]
        grid = nsp % NY == 0 and ntp == NX * CORES and nsp % ntp == 0
        cuts = columns % (HALVES * 128) == 0 and rows % (4 * WINDOW) == 0
        even = kn == 2 * HD and kn % 128 == 0 and qn == 4 * kn and pn == 2 * kn
        if grid and cuts and even:
            return fused(nsp // NY, ntp, *args)
        return local(*args)

    return body


def solution(mesh):
    return jax.shard_map(
        choose(mesh),
        mesh=mesh,
        in_specs=(
            P("sp", "tp"),
            P(),
            P("sp", "tp"),
            P("sp", "tp"),
            P("sp", "tp"),
            P("sp", "tp"),
            P("tp", None, None),
            P("tp"),
            P("tp", "sp"),
            P("tp", "sp"),
        ),
        out_specs=(P("sp", "tp"), P("tp", "sp")),
        check_vma=False,
    )
```

```python
import functools
import math

import jax
import jax.numpy as jnp
from jax import lax
from jax.experimental import pallas as pl
from jax.experimental.pallas import tpu as pltpu
from jax.sharding import PartitionSpec as P

HD = 64
WINDOW = 128
GRID_W = 64


norm_eps = 1e-06
rope_base = 10000.0
pool_reach = 8
neg_fill = -1e30


def with_halo(cells, sides, width):
    for axis, dim in sides:
        count = lax.axis_size(axis)
        ends = count - 1
        head = lax.slice_in_dim(cells, 0, width, axis=dim)
        tail = lax.slice_in_dim(cells, cells.shape[dim] - width, cells.shape[dim], axis=dim)
        cells = jnp.concatenate(
            [
                lax.ppermute(tail, axis, [(i, (i + 1) % count) for i in range(ends)]),
                cells,
                lax.ppermute(head, axis, [((i + 1) % count, i) for i in range(ends)]),
            ],
            axis=dim,
        )
    return cells


def rope_tables(positions, head_dim):
    n_freq = head_dim // 4
    freqs = rope_base ** (-jnp.arange(n_freq, dtype=jnp.float32) / n_freq)
    rows = (positions // GRID_W).astype(jnp.float32)
    columns = (positions % GRID_W).astype(jnp.float32)
    row_angle = rows[:, None] * freqs[None, :]
    col_angle = columns[:, None] * freqs[None, :]
    return (jnp.cos(row_angle), jnp.sin(row_angle), jnp.cos(col_angle), jnp.sin(col_angle))


def rotate_half(values, cosine, sine):
    middle = values.shape[-1] // 2
    first = values[..., :middle]
    second = values[..., middle:]
    return jnp.concatenate([first * cosine - second * sine, second * cosine + first * sine], -1)


def rotate_heads(values, tables, head_dim):
    rows_count = values.shape[0]
    shaped = values.astype(jnp.float32).reshape(rows_count, -1, head_dim)
    cos_r, sin_r, cos_c, sin_c = [table[:, None, :] for table in tables]
    split = head_dim // 2
    turned = jnp.concatenate(
        [
            rotate_half(shaped[..., :split], cos_r, sin_r),
            rotate_half(shaped[..., split:], cos_c, sin_c),
        ],
        -1,
    )
    return turned.reshape(rows_count, -1).astype(jnp.bfloat16)


def pool_group(extended, own, positions, half_width, seq_total):
    rows_count = own.shape[0]
    summed = jnp.zeros(own.shape, jnp.float32)
    counted = jnp.zeros((rows_count,), jnp.float32)
    for shift_by in range(-pool_reach, pool_reach):
        source = positions + shift_by
        inside = (
            (shift_by >= -half_width)
            & (shift_by < half_width)
            & (source >= 0)
            & (source < seq_total)
        )
        window_rows = extended[pool_reach + shift_by : pool_reach + shift_by + rows_count].astype(
            jnp.float32
        )
        summed = summed + jnp.where(inside[:, None], window_rows, 0.0)
        counted = counted + inside.astype(jnp.float32)
    return (summed / counted[:, None] - own.astype(jnp.float32)).astype(jnp.bfloat16)


def attend_block(queries, keys, values, sink, query_pos, key_pos, seq_total):
    scores = jnp.einsum(
        "qhgd,khd->hgqk", queries, keys, preferred_element_type=jnp.float32
    ) * HD ** (-0.5)
    valid = (
        (jnp.abs(query_pos[:, None] - key_pos[None, :]) <= WINDOW)
        & (key_pos >= 0)[None, :]
        & (key_pos < seq_total)[None, :]
    )
    scores = jnp.where(valid, scores, neg_fill)
    row_top = jnp.maximum(jnp.max(scores, -1), sink[:, :, None])
    exps = jnp.exp(scores - row_top[..., None])
    row_total = jnp.sum(exps, -1) + jnp.exp(sink[:, :, None] - row_top)
    weights = (exps / row_total[..., None]).astype(jnp.bfloat16)
    attended = jnp.einsum("hgqk,khd->qhgd", weights, values, preferred_element_type=jnp.float32)
    return (attended.astype(jnp.bfloat16), row_top + jnp.log(row_total))


def fetch_outputs(out_pool_weight, out_attn_weight):
    return (
        lax.all_gather(out_pool_weight, "sp", axis=1, tiled=True),
        lax.all_gather(out_attn_weight, "sp", axis=1, tiled=True),
    )


def local(
    tokens,
    norm_gain,
    query_weight,
    key_weight,
    value_weight,
    pool_in_weight,
    pool_mix_weight,
    sink_logit,
    out_pool_weight,
    out_attn_weight,
):
    whole = lax.all_gather(tokens, "tp", axis=1, tiled=True)
    wide = whole.astype(jnp.float32)
    normed = (
        wide * lax.rsqrt(jnp.mean(wide * wide, -1, keepdims=True) + norm_eps) * norm_gain
    ).astype(jnp.bfloat16)
    tok_rows = normed.shape[0]
    seq_total = tok_rows * lax.axis_size("sp")
    offset = lax.axis_index("sp") * tok_rows
    weights_in = (query_weight, key_weight, value_weight, pool_in_weight)
    pieces = (
        lax.all_gather(weights_in[0], "sp", axis=0, tiled=True),
        lax.all_gather(weights_in[1], "sp", axis=0, tiled=True),
        lax.all_gather(weights_in[2], "sp", axis=0, tiled=True),
        lax.all_gather(weights_in[3], "sp", axis=0, tiled=True),
    )
    sums = tuple((jnp.dot(normed, piece, preferred_element_type=jnp.float32) for piece in pieces))
    query, key, value, pool_input = [total.astype(jnp.bfloat16) for total in sums]
    positions = offset + jnp.arange(tok_rows, dtype=jnp.int32)
    tables = rope_tables(positions, HD)
    rot_query = rotate_heads(query, tables, HD)
    rot_key = rotate_heads(key, tables, HD)
    key_width = rot_key.shape[1]
    pool_ext = with_halo(pool_input, (("sp", 0),), pool_reach)
    pair_ext = with_halo(jnp.concatenate([rot_key, value], 1), (("sp", 0),), WINDOW)
    key_ext = pair_ext[:, :key_width]
    value_ext = pair_ext[:, key_width:]
    half_width = jnp.left_shift(jnp.int32(1), lax.axis_index("tp"))
    pooled = pool_group(pool_ext, pool_input, positions, half_width, seq_total)
    pool_out = jnp.dot(pooled, pool_mix_weight[0], preferred_element_type=jnp.float32).astype(
        jnp.bfloat16
    )
    heads_local = rot_query.shape[1] // HD
    kv_local = key_width // HD
    grp = heads_local // kv_local
    query_heads = rot_query.reshape(tok_rows, kv_local, grp, HD)
    key_heads = key_ext.reshape(-1, kv_local, HD)
    value_heads = value_ext.reshape(-1, kv_local, HD)
    sink = sink_logit.reshape(kv_local, grp)
    block_rows = min(tok_rows, 256)
    attended_parts = []
    log_parts = []
    for block_index in range(tok_rows // block_rows):
        start = block_index * block_rows
        query_pos = offset + start + jnp.arange(block_rows, dtype=jnp.int32)
        key_pos = offset + start - WINDOW + jnp.arange(block_rows + 2 * WINDOW, dtype=jnp.int32)
        attended_block, log_block = attend_block(
            query_heads[start : start + block_rows],
            key_heads[start : start + block_rows + 2 * WINDOW],
            value_heads[start : start + block_rows + 2 * WINDOW],
            sink,
            query_pos,
            key_pos,
            seq_total,
        )
        attended_parts.append(attended_block.reshape(block_rows, heads_local * HD))
        log_parts.append(log_block.reshape(heads_local, block_rows))
    attended = jnp.concatenate(attended_parts, 0)
    log_weight = jnp.concatenate(log_parts, 1)
    out_pool_full, out_attn_full = fetch_outputs(out_pool_weight, out_attn_weight)
    term = jnp.dot(pool_out, out_pool_full, preferred_element_type=jnp.float32)
    term = term + jnp.dot(attended, out_attn_full, preferred_element_type=jnp.float32)
    mixed = lax.psum_scatter(term.astype(jnp.bfloat16), "tp", scatter_dimension=1, tiled=True)
    return (mixed, log_weight)


NY = 2
NX = 2
CORES = 2
HALVES = 2
MESH = pl.DeviceIdType.MESH


def layer_kernel(
    nz,
    ntp,
    tok_ref,
    gain_ref,
    qw_ref,
    kw_ref,
    vw_ref,
    pw_ref,
    mix_ref,
    sink_ref,
    ow_ref,
    aw_ref,
    mixed_ref,
    log_ref,
    xg,
    normed,
    wg,
    wo,
    qrot,
    ext,
    act,
    part,
    rs1,
    tot,
    fin,
    cos_ref,
    sin_ref,
    mixb,
    gain,
    sinks,
    sink_own,
    sinkb,
    log_own,
    log_in,
    load_send,
    load_recv,
    w_send,
    w_recv,
    s_recv,
    o_recv,
    x_loc,
    x_send,
    x_recv,
    g_sem,
    m_send,
    m_recv,
    h_send,
    h_recv,
    r1_send,
    r1_recv,
    r2_send,
    r2_recv,
):
    sp, tp = lax.axis_index("sp"), lax.axis_index("tp")
    z, y = sp // NY, sp % NY
    x, c = tp // CORES, tp % CORES
    nsp = nz * NY
    block_of = z * NY + c
    group_of = x * CORES + y
    straight = c == y
    crossed = c != y
    rows, width = tok_ref.shape
    brow = qw_ref.shape[0]
    qn, kn, pn = qw_ref.shape[1], kw_ref.shape[1], pw_ref.shape[1]
    heads, kv_local = qn // HD, kn // HD
    grp = heads // kv_local
    gw = 2 * kn
    groups = wg.shape[0]
    pool_rows = ow_ref.shape[0]
    ohalf = wo.shape[3]
    seq_total = rows * nsp
    per_owner = nsp // ntp
    pieces = groups + HALVES

    def at(zz, yy, xx, cc):
        return (zz * NY + yy, xx * CORES + cc)

    def remote(src, dst, send, recv, target):
        return pltpu.make_async_remote_copy(
            src_ref=src,
            dst_ref=dst,
            send_sem=send,
            recv_sem=recv,
            device_id=target,
            device_id_type=MESH,
        )

    sibling = at(z, y, x, 1 - c)
    partner = at(z, 1 - y, x, 1 - c)

    def shard_rows(block):
        return pl.ds(pl.multiple_of(block * brow, brow), brow)

    def load_parts(p, block):
        if p == 0:
            return [
                (kw_ref, wg.at[0, shard_rows(block), pl.ds(0, kn)]),
                (vw_ref, wg.at[0, shard_rows(block), pl.ds(kn, kn)]),
            ]
        if p == 1:
            return [(pw_ref, wg.at[1, shard_rows(block)])]
        if p < groups:
            return [(qw_ref.at[:, pl.ds((p - 2) * gw, gw)], wg.at[p, shard_rows(block)])]
        h = p - groups
        cols = pl.ds(h * ohalf, ohalf)
        return [
            (ow_ref.at[:, cols], wo.at[block, h, pl.ds(0, pool_rows)]),
            (aw_ref.at[:, cols], wo.at[block, h, pl.ds(pool_rows, wo.shape[2] - pool_rows)]),
        ]

    def load_local(p):
        return [
            pltpu.make_async_copy(a, b, load_recv.at[p]) for a, b in load_parts(p, sp)
        ]

    def load_swap(p):
        return [
            remote(a, b, load_send.at[p // groups], load_recv.at[p], partner)
            for a, b in load_parts(p, sp)
        ]

    def piece_of(p, block):
        return wg.at[p, shard_rows(block)] if p < groups else wo.at[block, p - groups]

    def arrived(ref, sem):
        remote(ref, ref, load_send.at[0], sem, sibling).wait_recv()

    def departed(ref, sem):
        remote(ref, ref, sem, load_recv.at[0], sibling).wait_send()

    def load_wait(p):
        arrived(piece_of(p, block_of), load_recv.at[p])

    onward = (z + 1 < nz, z >= 1)
    middle = onward[0] & onward[1]
    outer = jnp.logical_not(middle)

    def w_copy(p, block, way):
        ref = piece_of(p, block)
        target = (at(z + 1, y, x, c), at(z - 1, y, x, c), sibling)[way]
        if way < 2:
            recv = w_recv.at[p, block // NY]
        elif p < groups:
            recv = s_recv.at[p]
        else:
            recv = o_recv.at[p - groups, block // NY]
        return remote(ref, ref, w_send.at[way, p // groups], recv, target)

    def send_own(p, ways):
        for way in ways:
            if way == 2:
                w_copy(p, block_of, 2).start()
            else:

                @pl.when(onward[way])
                def _():
                    w_copy(p, block_of, way).start()

    def relay(d, p):
        for way in range(2):
            source = (z - d, z + d)[way]
            block = source * NY + c

            @pl.when((source >= 0) & (source < nz))
            def _():
                w_copy(p, block, way).wait_recv()

                @pl.when(onward[way])
                def _():
                    w_copy(p, block, way).start()

                w_copy(p, block, 2).start()

    def stage(low, high, ok=None):
        if ok is not None:

            @pl.when(ok)
            def _():
                stage(low, high)

            return
        for turn_at in range(low, high):
            for p in range(groups):
                for role, when in ((straight, max(p - 1, 0)), (crossed, p)):
                    if when == turn_at:

                        @pl.when(role)
                        def _():
                            load_wait(p)
                            send_own(p, (0, 1, 2))

            for d in range(1, nz):
                for p in range(groups):
                    if turn_at == 2 * p + d:
                        relay(d, p)

    def gathered(p):
        arrived(wg.at[p, pl.ds(0, nz * brow)], s_recv.at[p])

    cut = rows // 4
    spans = (pl.ds(0, cut), pl.ds(cut, rows - cut))

    def token_copy(kind, r):
        target = (at(z, y, x, y), at(z, y, 1 - x, y), at(z, 1 - y, x, y))[kind]
        return remote(
            tok_ref.at[spans[r]], xg.at[tp, spans[r]], x_send.at[0], x_recv.at[tp, r], target
        )

    token_local = pltpu.make_async_copy(tok_ref, xg.at[tp], x_loc)

    def token_relay(k, r):
        slot = ((1 - x) if r == 0 else x) * CORES + k
        target = at(z, 1 - y, x, c) if r == 0 else at(z, y, 1 - x, c)
        ref = xg.at[slot, spans[r]]
        return remote(ref, ref, x_send.at[1], x_recv.at[slot, r], target)

    def token_wait(slot, r):
        arrived(xg.at[slot, spans[r]], x_recv.at[slot, r])

    mix_local = pltpu.make_async_copy(mix_ref.at[0], mixb, m_recv.at[0])
    mix_swap = remote(mix_ref.at[0], mixb, m_send.at[0], m_recv.at[0], partner)
    sink_swap = remote(sink_own, sinkb, m_send.at[1], m_recv.at[1], partner)

    gain_load = pltpu.make_async_copy(gain_ref, gain, g_sem.at[0])
    sink_load = pltpu.make_async_copy(sink_ref, sinks, g_sem.at[1])
    sink_load.start()
    gain_load.start()

    @pl.when(straight)
    def _():
        for p in range(groups):
            for copy in load_local(p):
                copy.start()
        token_local.start()

    barrier = pltpu.get_barrier_semaphore()
    met = jnp.int32(0)
    for flip in range(1, NY * NX * CORES):
        fy, fx, fc = flip // 4, (flip // 2) % 2, flip % 2
        pl.semaphore_signal(
            barrier,
            inc=1,
            device_id=at(
                z,
                1 - y if fy else y,
                1 - x if fx else x,
                1 - c if fc else c,
            ),
            device_id_type=MESH,
        )
        met = met + 1
    for ok, zz in ((onward[0], z + 1), (onward[1], z - 1)):
        met = met + CORES * ok.astype(jnp.int32)

        @pl.when(ok)
        def _():
            for cc in range(CORES):
                pl.semaphore_signal(
                    barrier, inc=1, device_id=at(zz, y, x, cc), device_id_type=MESH
                )

    ext[...] = jnp.zeros_like(ext)
    sink_load.wait()
    for head in range(heads):
        sink_own[head : head + 1, :] = jnp.full((1, 128), sinks[head], jnp.float32)

    @pl.when(straight)
    def _():
        sinkb[...] = sink_own[...]

    pl.semaphore_wait(barrier, met)

    @pl.when(straight)
    def _():
        for kind in (1, 2):
            for r in range(2):
                token_copy(kind, r if kind == 1 else 1 - r).start()
        mix_local.start()
        for p in range(groups, pieces):
            for copy in load_local(p):
                copy.start()

    @pl.when(crossed)
    def _():
        for r in range(2):
            token_copy(1, r).start()
            token_copy(0, r).start()
        for p in range(groups):
            for copy in load_swap(p):
                copy.start()
        token_copy(2, 1).start()
        token_copy(2, 0).start()
        sink_swap.start()
        mix_swap.start()
        for p in range(groups, pieces):
            for copy in load_swap(p):
                copy.start()

    stage(0, 1)

    half = HD // 4
    lane = lax.broadcasted_iota(jnp.int32, (rows, 128), 1)
    is_first = (lane % (2 * half)) < half
    position = block_of * rows + lax.broadcasted_iota(jnp.int32, (rows, 128), 0)
    place = jnp.where((lane % HD) < 2 * half, position // GRID_W, position % GRID_W)
    freqs = jnp.exp((lane % half).astype(jnp.float32) * (-math.log(rope_base) / half))
    angle = place.astype(jnp.float32) * freqs
    cos_ref[...] = jnp.cos(angle)
    sine = jnp.sin(angle)
    sin_ref[...] = jnp.where(is_first, -sine, sine)

    stage(1, 2)

    @pl.when(straight)
    def _():
        for k in range(CORES):
            token_relay(k, 0).wait_recv()
            token_relay(k, 0).start()

    @pl.when(crossed)
    def _():
        token_relay(c, 1).wait_recv()
        token_relay(c, 1).start()

    stage(2, nz)

    @pl.when(crossed)
    def _():
        token_relay(1 - c, 1).wait_recv()
        token_relay(1 - c, 1).start()

    stage(nz, nz + 2, middle)

    @pl.when(straight)
    def _():
        token_local.wait()
        for r in range(2):
            token_wait(x * CORES + (1 - c), r)
        for k in range(CORES):
            token_wait((1 - x) * CORES + k, 1)

    @pl.when(crossed)
    def _():
        for k in range(CORES):
            token_wait(x * CORES + k, 0)
            for r in range(2):
                token_wait((1 - x) * CORES + k, r)

    gain_load.wait()
    norm_rows = 64

    @pl.loop(0, rows // norm_rows)
    def _(i):
        take = pl.ds(pl.multiple_of(i * norm_rows, norm_rows), norm_rows)
        pieces_in = [xg[t, take, :].astype(jnp.float32) for t in range(ntp)]
        total = sum(jnp.sum(piece * piece, -1, keepdims=True) for piece in pieces_in)
        scale = lax.rsqrt(total / (width * ntp) + norm_eps)
        for t in range(ntp):
            cols = pl.ds(t * width, width)
            normed[take, cols] = (pieces_in[t] * scale * gain[:, cols]).astype(jnp.bfloat16)

    hrow = rows // 2
    lane_first = (lax.broadcasted_iota(jnp.int32, (hrow, 128), 1) % (2 * half)) < half

    def turn(values, low, factor):
        wide = values.astype(jnp.bfloat16).astype(jnp.float32)
        swapped = jnp.where(
            lane_first, pltpu.roll(wide, 128 - half, 1), pltpu.roll(wide, half, 1)
        )
        take = pl.ds(low, hrow)
        return ((wide * cos_ref[take] + swapped * sin_ref[take]) * factor).astype(jnp.bfloat16)

    def project(g, low):
        return jnp.dot(normed[pl.ds(low, hrow)], wg[g], preferred_element_type=jnp.float32)

    edge = 16
    has_next, has_prev = block_of + 1 < nsp, block_of >= 1
    next_at = at(z + c, y, x, 1 - c)
    prev_at = at(z + c - 1, y, x, 1 - c)

    def halo_copy(way, what):
        cols = pl.ds(0, gw) if what == 0 else pl.ds(gw, pn)
        count = WINDOW if what == 0 else edge
        if way == 0:
            src, dst = WINDOW + rows - count, WINDOW - count
        else:
            src, dst = WINDOW, WINDOW + rows
        return remote(
            ext.at[pl.ds(src, count), cols],
            ext.at[pl.ds(dst, count), cols],
            h_send.at[way, what],
            h_recv.at[way, what],
            next_at if way == 0 else prev_at,
        )

    def halo_send(what, done=False):
        for way, ok in ((0, has_next), (1, has_prev)):

            @pl.when(ok)
            def _():
                if done:
                    halo_copy(way, what).wait_send()
                else:
                    halo_copy(way, what).start()

    def halo_wait(what, near):
        for way, ok in ((0, has_prev), (1, has_next)):
            inside_chip = c == 1 if way == 0 else c == 0

            @pl.when(ok & (inside_chip if near else jnp.logical_not(inside_chip)))
            def _():
                halo_copy(way, what).wait_recv()

    gathered(0)
    for low in range(0, rows, hrow):
        pair = project(0, low)
        into = pl.ds(WINDOW + low, hrow)
        for col in range(0, kn, 128):
            ext[into, col : col + 128] = turn(pair[:, col : col + 128], low, 1.0)
        ext[into, kn:gw] = pair[:, kn:].astype(jnp.bfloat16)
    halo_send(0)

    stage(nz + 2, nz + 4, middle)
    stage(nz, nz + 2, outer)
    gathered(1)
    for low in range(0, rows, hrow):
        ext[pl.ds(WINDOW + low, hrow), gw : gw + pn] = project(1, low).astype(jnp.bfloat16)
    halo_send(1)
    stage(nz + 4, nz + 2 * groups, middle)
    behind = (z, nz - 1 - z)

    def own_out(ok, wait, ways, crowded):
        @pl.when(ok)
        def _():
            for p in range(groups, pieces):
                if wait:
                    load_wait(p)
                    w_copy(p, block_of, 2).start()
                for way in ways:

                    @pl.when(onward[way] & ((behind[way] > 1) == crowded))
                    def _():
                        w_copy(p, block_of, way).start()

    own_out(outer, True, (0, 1), False)
    span = 3 * WINDOW
    row_at = lax.broadcasted_iota(jnp.int32, (WINDOW, span), 0)
    key_at = lax.broadcasted_iota(jnp.int32, (WINDOW, span), 1)
    apart = key_at - row_at
    key_down = lax.broadcasted_iota(jnp.int32, (WINDOW, WINDOW), 0)
    query_over = lax.broadcasted_iota(jnp.int32, (WINDOW, WINDOW), 1)
    half_width = jnp.left_shift(jnp.int32(1), group_of)
    n_blocks = rows // WINDOW

    def inside_of(i):
        first = block_of * rows + (i - 1) * WINDOW
        return (key_at + first >= 0) & (key_at + first < seq_total)

    def attend(kv, i):
        q_at = pl.ds(pl.multiple_of(i * WINDOW, WINDOW), WINDOW)
        window = pl.ds(pl.multiple_of(i * WINDOW, WINDOW), span)
        first = block_of * rows + (i - 1) * WINDOW
        low = (key_down >= query_over) & (first >= 0)
        high = (key_down <= query_over) & (first + 2 * WINDOW < seq_total)
        keys = ext[window, kv * HD : (kv + 1) * HD]
        values = ext[window, kn + kv * HD : kn + (kv + 1) * HD].T
        weights, shares = [], []
        for g in range(grp):
            head = kv * grp + g
            query = qrot[q_at, head * HD : (head + 1) * HD]
            score = lax.dot_general(
                keys, query, (((1,), (1,)), ((), ())), preferred_element_type=jnp.float32
            )
            score = jnp.concatenate(
                [
                    jnp.where(low, score[:WINDOW], neg_fill),
                    score[WINDOW : 2 * WINDOW],
                    jnp.where(high, score[2 * WINDOW :], neg_fill),
                ],
                0,
            )
            sink = sinkb[head : head + 1, :]
            top = jnp.maximum(jnp.max(score, 0, keepdims=True), sink)
            exps = jnp.exp(score - top)
            total = jnp.sum(exps, 0, keepdims=True) + jnp.exp(sink - top)
            log_own[head : head + 1, q_at] = top + jnp.log(total)
            weights.append(exps.astype(jnp.bfloat16))
            shares.append(1.0 / total)
        out = jnp.dot(values, jnp.concatenate(weights, 1), preferred_element_type=jnp.float32)
        outs = [out[:, g * WINDOW : (g + 1) * WINDOW] * shares[g] for g in range(grp)]
        col = pn + kv * grp * HD
        act[q_at, col : col + grp * HD] = jnp.concatenate(outs, 0).T.astype(jnp.bfloat16)

    late = jnp.where(c == 0, 0, n_blocks - 1)
    early = n_blocks - 1 - late

    def attend_early(kv):
        for i in range(1, n_blocks - 1):
            attend(kv, i)
        attend(kv, early)

    def queries(kv, g):
        for low in range(0, rows, hrow):
            both = project(g, low)
            for col in range(0, gw, 128):
                at_col = kv * gw + col
                qrot[pl.ds(low, hrow), at_col : at_col + 128] = turn(
                    both[:, col : col + 128], low, HD ** -0.5
                )

    @pl.when(crossed)
    def _():
        remote(sink_own, sinkb, m_send.at[1], m_recv.at[1], partner).wait_recv()

    def pool(i):
        q_at = pl.ds(pl.multiple_of(i * WINDOW, WINDOW), WINDOW)
        window = pl.ds(pl.multiple_of(i * WINDOW, WINDOW), span)
        own_at = pl.ds(pl.multiple_of((i + 1) * WINDOW, WINDOW), WINDOW)
        band = inside_of(i) & (apart >= WINDOW - half_width) & (apart < WINDOW + half_width)
        band_f = band.astype(jnp.float32)
        counted = jnp.sum(band_f, -1, keepdims=True)
        summed = jnp.dot(
            band_f.astype(jnp.bfloat16),
            ext[window, gw : gw + pn],
            preferred_element_type=jnp.float32,
        )
        own_pool = ext[own_at, gw : gw + pn]
        pooled = (summed / counted - own_pool.astype(jnp.float32)).astype(jnp.bfloat16)
        act[q_at, 0:pn] = jnp.dot(
            pooled, mixb[...], preferred_element_type=jnp.float32
        ).astype(jnp.bfloat16)

    halo_wait(1, True)

    @pl.when(straight)
    def _():
        mix_local.wait()

    @pl.when(crossed)
    def _():
        mix_swap.wait_recv()

    for i in range(1, n_blocks - 1):
        pool(i)
    pool(early)

    stage(nz + 2, nz + 4, outer)
    gathered(2)
    queries(0, 2)
    halo_wait(0, True)
    own_out(middle, True, (0, 1), False)
    attend_early(0)
    own_out(middle, False, (0, 1), True)
    stage(nz + 4, nz + 2 * groups, outer)
    halo_wait(0, False)
    attend(0, late)
    halo_wait(1, False)
    pool(late)

    def r1_copy(block, h, rh):
        take = pl.ds(rh * hrow, hrow)
        return remote(
            part.at[h, block, take],
            rs1.at[h, block, take],
            r1_send.at[h],
            r1_recv.at[h, block, rh],
            at(z, 1 - y, x, c),
        )

    def r2_copy(block, h, rh):
        take = pl.ds(rh * hrow, hrow)
        owner = block // per_owner
        slot = block % per_owner
        side = jnp.where(owner // CORES == x, 0, 1)
        return remote(
            tot.at[h, block, take],
            fin.at[side, h, slot, take],
            r2_send.at[h],
            r2_recv.at[side],
            (sp, owner),
        )

    def each_block(d, lead, body):
        parity = y if lead == 0 else 1 - y
        for way in range(1 if d == 0 else 2):
            source = z + (2 * way - 1) * d

            @pl.when((source >= 0) & (source < nz))
            def _():
                body(source * NY + parity)

    def compute(d, h, lead, halves=(0, 1)):
        def body(block):
            if halves[0] == 0:

                @pl.when(crossed if lead == 0 else straight)
                def _():
                    w_copy(groups + h, block, 2).wait_recv()

            take = pl.ds(halves[0] * hrow, len(halves) * hrow)
            part[h, block, take] = jnp.dot(
                act[take], wo[block, h], preferred_element_type=jnp.float32
            ).astype(jnp.bfloat16)

            @pl.when(crossed)
            def _():
                for rh in halves:
                    r1_copy(block, h, rh).start()

        each_block(d, lead, body)

    def join(d, h):
        def body(block):
            for rh in range(2):
                take = pl.ds(rh * hrow, hrow)
                r1_copy(block, h, rh).wait_recv()
                tot[h, block, take] = (
                    part[h, block, take].astype(jnp.float32)
                    + rs1[h, block, take].astype(jnp.float32)
                ).astype(jnp.bfloat16)

                @pl.when(block // per_owner != tp)
                def _():
                    r2_copy(block, h, rh).start()

        @pl.when(straight)
        def _():
            for lead in range(2):
                each_block(d, lead, body)

    gathered(3)
    queries(1, 3)
    log_swap = remote(log_own, log_in, m_send.at[2], m_recv.at[2], partner)

    for rh in range(2):
        for i in range(rh * n_blocks // 2, (rh + 1) * n_blocks // 2):
            attend(1, i)
        for h in range(HALVES):
            for lead in range(2):
                compute(0, h, lead, (rh,))

    @pl.when(crossed)
    def _():
        log_swap.start()

    def pass_on(d, h, ok):
        @pl.when(ok)
        def _():
            relay(d, groups + h)

    order = [(d, h) for d in range(nz) for h in range(HALVES)]

    def advance(n):
        d, h = order[n]
        compute(d, h, 0)
        pass_on(d, h, outer & crossed)
        if n + 1 < len(order):
            pass_on(*order[n + 1], outer & straight)
        compute(d, h, 1)

    for h in range(HALVES):
        pass_on(1, h, middle)
    joined = 0
    for n in range(HALVES, len(order)):
        if n == HALVES:
            pass_on(*order[n], outer & straight)
        advance(n)
        if n == 2 * HALVES - 1:
            join(*order[0])
            for far in range(2, nz):
                for h in range(HALVES):
                    pass_on(far, h, middle)
            join(*order[1])
            joined = 2
        elif n >= 2 * HALVES:
            while joined < n:
                join(*order[joined])
                joined += 1
    for n in range(joined, len(order)):
        join(*order[n])

    @pl.when(straight)
    def _():
        log_ref[...] = log_own[...]

    @pl.when(crossed)
    def _():
        log_swap.wait_recv()
        log_ref[...] = log_in[...]

    arrived(fin.at[1], r2_recv.at[1])

    @pl.when(crossed)
    def _():
        arrived(fin.at[0], r2_recv.at[0])

    for slot in range(per_owner):
        for h in range(HALVES):
            low = (slot * HALVES + h) * ohalf
            far = fin[1, h, slot].astype(jnp.float32)

            @pl.when(straight)
            def _():
                near = tot[h, tp * per_owner + slot].astype(jnp.float32)
                mixed_ref[:, low : low + ohalf] = (near + far).astype(jnp.bfloat16)

            @pl.when(crossed)
            def _():
                near = fin[0, h, slot].astype(jnp.float32)
                mixed_ref[:, low : low + ohalf] = (near + far).astype(jnp.bfloat16)

    def all_sent(way, count):
        departed(wg.at[pl.ds(0, groups), pl.ds(0, count * brow)], w_send.at[way, 0])
        departed(wo.at[pl.ds(0, count)], w_send.at[way, 1])

    all_sent(2, nz)
    for count in range(1, nz):
        for way, passed in ((0, z + 1), (1, nz - z)):

            @pl.when(onward[way] & (passed == count))
            def _():
                all_sent(way, count)

    halo_send(0, done=True)
    halo_send(1, done=True)

    @pl.when(straight)
    def _():
        departed(xg.at[pl.ds(0, 2)], x_send.at[0])
        departed(xg.at[pl.ds(0, CORES), spans[0]], x_send.at[1])
        for h in range(HALVES):
            departed(tot.at[h, pl.ds(0, nsp - per_owner)], r2_send.at[h])

    @pl.when(crossed)
    def _():
        departed(xg.at[pl.ds(0, 3)], x_send.at[0])
        departed(xg.at[pl.ds(0, CORES), spans[1]], x_send.at[1])
        departed(wg.at[pl.ds(0, groups), pl.ds(0, brow)], load_send.at[0])
        departed(wo.at[0], load_send.at[1])
        mix_swap.wait_send()
        sink_swap.wait_send()
        log_swap.wait_send()
        for h in range(HALVES):
            departed(part.at[h], r1_send.at[h])


def place_kernel(mixed_ref, log_ref, mixed_out, log_out, sems):
    copies = [
        pltpu.make_async_copy(mixed_ref, mixed_out, sems.at[0]),
        pltpu.make_async_copy(log_ref, log_out, sems.at[1]),
    ]
    for copy in copies:
        copy.start()
    for copy in copies:
        copy.wait()


def fused(
    nz,
    ntp,
    tokens,
    norm_gain,
    query_weight,
    key_weight,
    value_weight,
    pool_in_weight,
    pool_mix_weight,
    sink_logit,
    out_pool_weight,
    out_attn_weight,
):
    rows, width = tokens.shape
    nsp = nz * NY
    dim = width * ntp
    qn, kn, pn = query_weight.shape[1], key_weight.shape[1], pool_in_weight.shape[1]
    fan = out_pool_weight.shape[0] + out_attn_weight.shape[0]
    ohalf = out_pool_weight.shape[1] // HALVES
    heads = sink_logit.shape[0]
    gw = 2 * kn
    groups = (qn + 2 * kn + pn) // gw
    pieces = groups + HALVES
    hbm = pl.BlockSpec(memory_space=pl.ANY)
    vmem = pl.BlockSpec(memory_space=pltpu.VMEM)
    dma = pltpu.SemaphoreType.DMA
    bf16 = jnp.bfloat16
    f32 = jnp.float32
    per_owner = nsp // ntp
    outs = (
        jax.ShapeDtypeStruct((rows, width), bf16),
        jax.ShapeDtypeStruct((heads, rows), f32),
    )
    mixed, logs = pl.pallas_call(
        functools.partial(layer_kernel, nz, ntp),
        out_shape=outs,
        in_specs=[hbm] * 10,
        out_specs=(vmem, vmem),
        scratch_shapes=[
            pltpu.VMEM((ntp, rows, width), bf16),
            pltpu.VMEM((rows, dim), bf16),
            pltpu.VMEM((groups, dim, gw), bf16),
            pltpu.VMEM((nsp, HALVES, fan, ohalf), bf16),
            pltpu.VMEM((rows, qn), bf16),
            pltpu.VMEM((rows + 2 * WINDOW, gw + pn), bf16),
            pltpu.VMEM((rows, fan), bf16),
            pltpu.VMEM((HALVES, nsp, rows, ohalf), bf16),
            pltpu.VMEM((HALVES, nsp, rows, ohalf), bf16),
            pltpu.VMEM((HALVES, nsp, rows, ohalf), bf16),
            pltpu.VMEM((2, HALVES, per_owner, rows, ohalf), bf16),
            pltpu.VMEM((rows, 128), f32),
            pltpu.VMEM((rows, 128), f32),
            pltpu.VMEM((pn, pn), bf16),
            pltpu.VMEM((1, dim), f32),
            pltpu.SMEM((heads,), f32),
            pltpu.VMEM((heads, 128), f32),
            pltpu.VMEM((heads, 128), f32),
            pltpu.VMEM((heads, rows), f32),
            pltpu.VMEM((heads, rows), f32),
            dma((2,)),
            dma((pieces,)),
            dma((3, 2)),
            dma((pieces, nz)),
            dma((groups,)),
            dma((HALVES, nz)),
            dma,
            dma((2,)),
            dma((ntp, 2)),
            dma((2,)),
            dma((3,)),
            dma((3,)),
            dma((2, 2)),
            dma((2, 2)),
            dma((HALVES,)),
            dma((HALVES, nsp, 2)),
            dma((HALVES,)),
            dma((2,)),
        ],
        compiler_params=pltpu.CompilerParams(
            collective_id=0, has_side_effects=True, vmem_limit_bytes=56 << 20
        ),
    )(
        tokens,
        norm_gain[None, :],
        query_weight,
        key_weight,
        value_weight,
        pool_in_weight,
        pool_mix_weight,
        sink_logit,
        out_pool_weight,
        out_attn_weight,
    )
    return pl.pallas_call(
        place_kernel,
        out_shape=outs,
        in_specs=[vmem, vmem],
        out_specs=(hbm, hbm),
        scratch_shapes=[dma((2,))],
    )(mixed, logs)


def choose(mesh):
    nsp, ntp = mesh.shape["sp"], mesh.shape["tp"]

    def body(*args):
        rows = args[0].shape[0]
        qn, kn, pn = args[2].shape[1], args[3].shape[1], args[5].shape[1]
        columns = args[8].shape[1]
        grid = nsp % NY == 0 and ntp == NX * CORES and nsp % ntp == 0
        cuts = columns % (HALVES * 128) == 0 and rows % (4 * WINDOW) == 0
        even = kn == 2 * HD and kn % 128 == 0 and qn == 4 * kn and pn == 2 * kn
        if grid and cuts and even:
            return fused(nsp // NY, ntp, *args)
        return local(*args)

    return body


def solution(mesh):
    return jax.shard_map(
        choose(mesh),
        mesh=mesh,
        in_specs=(
            P("sp", "tp"),
            P(),
            P("sp", "tp"),
            P("sp", "tp"),
            P("sp", "tp"),
            P("sp", "tp"),
            P("tp", None, None),
            P("tp"),
            P("tp", "sp"),
            P("tp", "sp"),
        ),
        out_specs=(P("sp", "tp"), P("tp", "sp")),
        check_vma=False,
    )
```

```python
import functools
import math

import jax
import jax.numpy as jnp
from jax import lax
from jax.experimental import pallas as pl
from jax.experimental.pallas import tpu as pltpu
from jax.sharding import PartitionSpec as P

HD = 64
WINDOW = 128
GRID_W = 64


norm_eps = 1e-06
rope_base = 10000.0
pool_reach = 8
neg_fill = -1e30


def with_halo(cells, sides, width):
    for axis, dim in sides:
        count = lax.axis_size(axis)
        ends = count - 1
        head = lax.slice_in_dim(cells, 0, width, axis=dim)
        tail = lax.slice_in_dim(cells, cells.shape[dim] - width, cells.shape[dim], axis=dim)
        cells = jnp.concatenate(
            [
                lax.ppermute(tail, axis, [(i, (i + 1) % count) for i in range(ends)]),
                cells,
                lax.ppermute(head, axis, [((i + 1) % count, i) for i in range(ends)]),
            ],
            axis=dim,
        )
    return cells


def rope_tables(positions, head_dim):
    n_freq = head_dim // 4
    freqs = rope_base ** (-jnp.arange(n_freq, dtype=jnp.float32) / n_freq)
    rows = (positions // GRID_W).astype(jnp.float32)
    columns = (positions % GRID_W).astype(jnp.float32)
    row_angle = rows[:, None] * freqs[None, :]
    col_angle = columns[:, None] * freqs[None, :]
    return (jnp.cos(row_angle), jnp.sin(row_angle), jnp.cos(col_angle), jnp.sin(col_angle))


def rotate_half(values, cosine, sine):
    middle = values.shape[-1] // 2
    first = values[..., :middle]
    second = values[..., middle:]
    return jnp.concatenate([first * cosine - second * sine, second * cosine + first * sine], -1)


def rotate_heads(values, tables, head_dim):
    rows_count = values.shape[0]
    shaped = values.astype(jnp.float32).reshape(rows_count, -1, head_dim)
    cos_r, sin_r, cos_c, sin_c = [table[:, None, :] for table in tables]
    split = head_dim // 2
    turned = jnp.concatenate(
        [
            rotate_half(shaped[..., :split], cos_r, sin_r),
            rotate_half(shaped[..., split:], cos_c, sin_c),
        ],
        -1,
    )
    return turned.reshape(rows_count, -1).astype(jnp.bfloat16)


def pool_group(extended, own, positions, half_width, seq_total):
    rows_count = own.shape[0]
    summed = jnp.zeros(own.shape, jnp.float32)
    counted = jnp.zeros((rows_count,), jnp.float32)
    for shift_by in range(-pool_reach, pool_reach):
        source = positions + shift_by
        inside = (
            (shift_by >= -half_width)
            & (shift_by < half_width)
            & (source >= 0)
            & (source < seq_total)
        )
        window_rows = extended[pool_reach + shift_by : pool_reach + shift_by + rows_count].astype(
            jnp.float32
        )
        summed = summed + jnp.where(inside[:, None], window_rows, 0.0)
        counted = counted + inside.astype(jnp.float32)
    return (summed / counted[:, None] - own.astype(jnp.float32)).astype(jnp.bfloat16)


def attend_block(queries, keys, values, sink, query_pos, key_pos, seq_total):
    scores = jnp.einsum(
        "qhgd,khd->hgqk", queries, keys, preferred_element_type=jnp.float32
    ) * HD ** (-0.5)
    valid = (
        (jnp.abs(query_pos[:, None] - key_pos[None, :]) <= WINDOW)
        & (key_pos >= 0)[None, :]
        & (key_pos < seq_total)[None, :]
    )
    scores = jnp.where(valid, scores, neg_fill)
    row_top = jnp.maximum(jnp.max(scores, -1), sink[:, :, None])
    exps = jnp.exp(scores - row_top[..., None])
    row_total = jnp.sum(exps, -1) + jnp.exp(sink[:, :, None] - row_top)
    weights = (exps / row_total[..., None]).astype(jnp.bfloat16)
    attended = jnp.einsum("hgqk,khd->qhgd", weights, values, preferred_element_type=jnp.float32)
    return (attended.astype(jnp.bfloat16), row_top + jnp.log(row_total))


def fetch_outputs(out_pool_weight, out_attn_weight):
    return (
        lax.all_gather(out_pool_weight, "sp", axis=1, tiled=True),
        lax.all_gather(out_attn_weight, "sp", axis=1, tiled=True),
    )


def local(
    tokens,
    norm_gain,
    query_weight,
    key_weight,
    value_weight,
    pool_in_weight,
    pool_mix_weight,
    sink_logit,
    out_pool_weight,
    out_attn_weight,
):
    whole = lax.all_gather(tokens, "tp", axis=1, tiled=True)
    wide = whole.astype(jnp.float32)
    normed = (
        wide * lax.rsqrt(jnp.mean(wide * wide, -1, keepdims=True) + norm_eps) * norm_gain
    ).astype(jnp.bfloat16)
    tok_rows = normed.shape[0]
    seq_total = tok_rows * lax.axis_size("sp")
    offset = lax.axis_index("sp") * tok_rows
    weights_in = (query_weight, key_weight, value_weight, pool_in_weight)
    pieces = (
        lax.all_gather(weights_in[0], "sp", axis=0, tiled=True),
        lax.all_gather(weights_in[1], "sp", axis=0, tiled=True),
        lax.all_gather(weights_in[2], "sp", axis=0, tiled=True),
        lax.all_gather(weights_in[3], "sp", axis=0, tiled=True),
    )
    sums = tuple((jnp.dot(normed, piece, preferred_element_type=jnp.float32) for piece in pieces))
    query, key, value, pool_input = [total.astype(jnp.bfloat16) for total in sums]
    positions = offset + jnp.arange(tok_rows, dtype=jnp.int32)
    tables = rope_tables(positions, HD)
    rot_query = rotate_heads(query, tables, HD)
    rot_key = rotate_heads(key, tables, HD)
    key_width = rot_key.shape[1]
    pool_ext = with_halo(pool_input, (("sp", 0),), pool_reach)
    pair_ext = with_halo(jnp.concatenate([rot_key, value], 1), (("sp", 0),), WINDOW)
    key_ext = pair_ext[:, :key_width]
    value_ext = pair_ext[:, key_width:]
    half_width = jnp.left_shift(jnp.int32(1), lax.axis_index("tp"))
    pooled = pool_group(pool_ext, pool_input, positions, half_width, seq_total)
    pool_out = jnp.dot(pooled, pool_mix_weight[0], preferred_element_type=jnp.float32).astype(
        jnp.bfloat16
    )
    heads_local = rot_query.shape[1] // HD
    kv_local = key_width // HD
    grp = heads_local // kv_local
    query_heads = rot_query.reshape(tok_rows, kv_local, grp, HD)
    key_heads = key_ext.reshape(-1, kv_local, HD)
    value_heads = value_ext.reshape(-1, kv_local, HD)
    sink = sink_logit.reshape(kv_local, grp)
    block_rows = min(tok_rows, 256)
    attended_parts = []
    log_parts = []
    for block_index in range(tok_rows // block_rows):
        start = block_index * block_rows
        query_pos = offset + start + jnp.arange(block_rows, dtype=jnp.int32)
        key_pos = offset + start - WINDOW + jnp.arange(block_rows + 2 * WINDOW, dtype=jnp.int32)
        attended_block, log_block = attend_block(
            query_heads[start : start + block_rows],
            key_heads[start : start + block_rows + 2 * WINDOW],
            value_heads[start : start + block_rows + 2 * WINDOW],
            sink,
            query_pos,
            key_pos,
            seq_total,
        )
        attended_parts.append(attended_block.reshape(block_rows, heads_local * HD))
        log_parts.append(log_block.reshape(heads_local, block_rows))
    attended = jnp.concatenate(attended_parts, 0)
    log_weight = jnp.concatenate(log_parts, 1)
    out_pool_full, out_attn_full = fetch_outputs(out_pool_weight, out_attn_weight)
    term = jnp.dot(pool_out, out_pool_full, preferred_element_type=jnp.float32)
    term = term + jnp.dot(attended, out_attn_full, preferred_element_type=jnp.float32)
    mixed = lax.psum_scatter(term.astype(jnp.bfloat16), "tp", scatter_dimension=1, tiled=True)
    return (mixed, log_weight)


NY = 2
NX = 2
CORES = 2
HALVES = 2
MESH = pl.DeviceIdType.MESH


def layer_kernel(
    nz,
    ntp,
    tok_ref,
    gain_ref,
    qw_ref,
    kw_ref,
    vw_ref,
    pw_ref,
    mix_ref,
    sink_ref,
    ow_ref,
    aw_ref,
    mixed_ref,
    log_ref,
    xg,
    normed,
    wg,
    wo,
    qrot,
    ext,
    act,
    part,
    rs1,
    tot,
    fin,
    cos_ref,
    sin_ref,
    mixb,
    gain,
    sinks,
    sink_own,
    sinkb,
    log_own,
    log_in,
    load_send,
    load_recv,
    w_send,
    w_recv,
    s_recv,
    o_recv,
    x_loc,
    x_send,
    x_recv,
    g_sem,
    m_send,
    m_recv,
    h_send,
    h_recv,
    r1_send,
    r1_recv,
    r2_send,
    r2_recv,
):
    sp, tp = lax.axis_index("sp"), lax.axis_index("tp")
    z, y = sp // NY, sp % NY
    x, c = tp // CORES, tp % CORES
    nsp = nz * NY
    block_of = z * NY + c
    group_of = x * CORES + y
    straight = c == y
    crossed = c != y
    rows, width = tok_ref.shape
    brow = qw_ref.shape[0]
    qn, kn, pn = qw_ref.shape[1], kw_ref.shape[1], pw_ref.shape[1]
    heads, kv_local = qn // HD, kn // HD
    grp = heads // kv_local
    gw = 2 * kn
    groups = wg.shape[0]
    pool_rows = ow_ref.shape[0]
    ohalf = wo.shape[3]
    seq_total = rows * nsp
    per_owner = nsp // ntp
    pieces = groups + HALVES

    def at(zz, yy, xx, cc):
        return (zz * NY + yy, xx * CORES + cc)

    def remote(src, dst, send, recv, target):
        return pltpu.make_async_remote_copy(
            src_ref=src,
            dst_ref=dst,
            send_sem=send,
            recv_sem=recv,
            device_id=target,
            device_id_type=MESH,
        )

    sibling = at(z, y, x, 1 - c)
    partner = at(z, 1 - y, x, 1 - c)

    def shard_rows(block):
        return pl.ds(pl.multiple_of(block * brow, brow), brow)

    def load_parts(p, block):
        if p == 0:
            return [
                (kw_ref, wg.at[0, shard_rows(block), pl.ds(0, kn)]),
                (vw_ref, wg.at[0, shard_rows(block), pl.ds(kn, kn)]),
            ]
        if p == 1:
            return [(pw_ref, wg.at[1, shard_rows(block)])]
        if p < groups:
            return [(qw_ref.at[:, pl.ds((p - 2) * gw, gw)], wg.at[p, shard_rows(block)])]
        h = p - groups
        cols = pl.ds(h * ohalf, ohalf)
        return [
            (ow_ref.at[:, cols], wo.at[block, h, pl.ds(0, pool_rows)]),
            (aw_ref.at[:, cols], wo.at[block, h, pl.ds(pool_rows, wo.shape[2] - pool_rows)]),
        ]

    def load_local(p):
        return [
            pltpu.make_async_copy(a, b, load_recv.at[p]) for a, b in load_parts(p, sp)
        ]

    def load_swap(p):
        return [
            remote(a, b, load_send.at[p // groups], load_recv.at[p], partner)
            for a, b in load_parts(p, sp)
        ]

    def piece_of(p, block):
        return wg.at[p, shard_rows(block)] if p < groups else wo.at[block, p - groups]

    def arrived(ref, sem):
        remote(ref, ref, load_send.at[0], sem, sibling).wait_recv()

    def departed(ref, sem):
        remote(ref, ref, sem, load_recv.at[0], sibling).wait_send()

    def load_wait(p):
        arrived(piece_of(p, block_of), load_recv.at[p])

    onward = (z + 1 < nz, z >= 1)
    middle = onward[0] & onward[1]
    outer = jnp.logical_not(middle)

    def w_copy(p, block, way):
        ref = piece_of(p, block)
        target = (at(z + 1, y, x, c), at(z - 1, y, x, c), sibling)[way]
        if way < 2:
            recv = w_recv.at[p, block // NY]
        elif p < groups:
            recv = s_recv.at[p]
        else:
            recv = o_recv.at[p - groups, block // NY]
        return remote(ref, ref, w_send.at[way, p // groups], recv, target)

    def send_own(p, ways):
        for way in ways:
            if way == 2:
                w_copy(p, block_of, 2).start()
            else:

                @pl.when(onward[way])
                def _():
                    w_copy(p, block_of, way).start()

    def relay(d, p):
        for way in range(2):
            source = (z - d, z + d)[way]
            block = source * NY + c

            @pl.when((source >= 0) & (source < nz))
            def _():
                w_copy(p, block, way).wait_recv()

                @pl.when(onward[way])
                def _():
                    w_copy(p, block, way).start()

                w_copy(p, block, 2).start()

    def stage(low, high, ok=None):
        if ok is not None:

            @pl.when(ok)
            def _():
                stage(low, high)

            return
        for turn_at in range(low, high):
            for p in range(groups):
                for role, when in ((straight, max(p - 1, 0)), (crossed, p)):
                    if when == turn_at:

                        @pl.when(role)
                        def _():
                            load_wait(p)
                            send_own(p, (0, 1, 2))

            for d in range(1, nz):
                for p in range(groups):
                    if turn_at == 2 * p + d:
                        relay(d, p)

    def gathered(p):
        arrived(wg.at[p, pl.ds(0, nz * brow)], s_recv.at[p])

    cut = rows // 4
    spans = (pl.ds(0, cut), pl.ds(cut, rows - cut))

    def token_copy(kind, r):
        target = (at(z, y, x, y), at(z, y, 1 - x, y), at(z, 1 - y, x, y))[kind]
        return remote(
            tok_ref.at[spans[r]], xg.at[tp, spans[r]], x_send.at[0], x_recv.at[tp, r], target
        )

    token_local = pltpu.make_async_copy(tok_ref, xg.at[tp], x_loc)

    def token_relay(k, r):
        slot = ((1 - x) if r == 0 else x) * CORES + k
        target = at(z, 1 - y, x, c) if r == 0 else at(z, y, 1 - x, c)
        ref = xg.at[slot, spans[r]]
        return remote(ref, ref, x_send.at[1], x_recv.at[slot, r], target)

    def token_wait(slot, r):
        arrived(xg.at[slot, spans[r]], x_recv.at[slot, r])

    mix_local = pltpu.make_async_copy(mix_ref.at[0], mixb, m_recv.at[0])
    mix_swap = remote(mix_ref.at[0], mixb, m_send.at[0], m_recv.at[0], partner)
    sink_swap = remote(sink_own, sinkb, m_send.at[1], m_recv.at[1], partner)

    gain_load = pltpu.make_async_copy(gain_ref, gain, g_sem.at[0])
    sink_load = pltpu.make_async_copy(sink_ref, sinks, g_sem.at[1])
    sink_load.start()
    gain_load.start()

    @pl.when(straight)
    def _():
        for p in range(groups):
            for copy in load_local(p):
                copy.start()
        token_local.start()

    barrier = pltpu.get_barrier_semaphore()
    met = jnp.int32(0)
    for flip in range(1, NY * NX * CORES):
        fy, fx, fc = flip // 4, (flip // 2) % 2, flip % 2
        pl.semaphore_signal(
            barrier,
            inc=1,
            device_id=at(
                z,
                1 - y if fy else y,
                1 - x if fx else x,
                1 - c if fc else c,
            ),
            device_id_type=MESH,
        )
        met = met + 1
    for ok, zz in ((onward[0], z + 1), (onward[1], z - 1)):
        met = met + CORES * ok.astype(jnp.int32)

        @pl.when(ok)
        def _():
            for cc in range(CORES):
                pl.semaphore_signal(
                    barrier, inc=1, device_id=at(zz, y, x, cc), device_id_type=MESH
                )

    ext[...] = jnp.zeros_like(ext)
    sink_load.wait()
    for head in range(heads):
        sink_own[head : head + 1, :] = jnp.full((1, 128), sinks[head], jnp.float32)

    @pl.when(straight)
    def _():
        sinkb[...] = sink_own[...]

    pl.semaphore_wait(barrier, met)

    @pl.when(straight)
    def _():
        for kind in (1, 2):
            for r in range(2):
                token_copy(kind, r if kind == 1 else 1 - r).start()
        mix_local.start()
        for p in range(groups, pieces):
            for copy in load_local(p):
                copy.start()

    @pl.when(crossed)
    def _():
        for r in range(2):
            token_copy(1, r).start()
            token_copy(0, r).start()
        for p in range(groups):
            for copy in load_swap(p):
                copy.start()
        token_copy(2, 1).start()
        token_copy(2, 0).start()
        sink_swap.start()
        mix_swap.start()
        for p in range(groups, pieces):
            for copy in load_swap(p):
                copy.start()

    stage(0, 1)

    half = HD // 4
    lane = lax.broadcasted_iota(jnp.int32, (rows, 128), 1)
    is_first = (lane % (2 * half)) < half
    position = block_of * rows + lax.broadcasted_iota(jnp.int32, (rows, 128), 0)
    place = jnp.where((lane % HD) < 2 * half, position // GRID_W, position % GRID_W)
    freqs = jnp.exp((lane % half).astype(jnp.float32) * (-math.log(rope_base) / half))
    angle = place.astype(jnp.float32) * freqs
    cos_ref[...] = jnp.cos(angle)
    sine = jnp.sin(angle)
    sin_ref[...] = jnp.where(is_first, -sine, sine)

    stage(1, 2)

    @pl.when(straight)
    def _():
        for k in range(CORES):
            token_relay(k, 0).wait_recv()
            token_relay(k, 0).start()

    @pl.when(crossed)
    def _():
        token_relay(c, 1).wait_recv()
        token_relay(c, 1).start()

    stage(2, nz)

    @pl.when(crossed)
    def _():
        token_relay(1 - c, 1).wait_recv()
        token_relay(1 - c, 1).start()

    stage(nz, nz + 2, middle)

    @pl.when(straight)
    def _():
        token_local.wait()
        for r in range(2):
            token_wait(x * CORES + (1 - c), r)
        for k in range(CORES):
            token_wait((1 - x) * CORES + k, 1)

    @pl.when(crossed)
    def _():
        for k in range(CORES):
            token_wait(x * CORES + k, 0)
            for r in range(2):
                token_wait((1 - x) * CORES + k, r)

    gain_load.wait()
    norm_rows = 64

    @pl.loop(0, rows // norm_rows)
    def _(i):
        take = pl.ds(pl.multiple_of(i * norm_rows, norm_rows), norm_rows)
        pieces_in = [xg[t, take, :].astype(jnp.float32) for t in range(ntp)]
        total = sum(jnp.sum(piece * piece, -1, keepdims=True) for piece in pieces_in)
        scale = lax.rsqrt(total / (width * ntp) + norm_eps)
        for t in range(ntp):
            cols = pl.ds(t * width, width)
            normed[take, cols] = (pieces_in[t] * scale * gain[:, cols]).astype(jnp.bfloat16)

    hrow = rows // 2
    lane_first = (lax.broadcasted_iota(jnp.int32, (hrow, 128), 1) % (2 * half)) < half

    def turn(values, low, factor):
        wide = values.astype(jnp.bfloat16).astype(jnp.float32)
        swapped = jnp.where(
            lane_first, pltpu.roll(wide, 128 - half, 1), pltpu.roll(wide, half, 1)
        )
        take = pl.ds(low, hrow)
        return ((wide * cos_ref[take] + swapped * sin_ref[take]) * factor).astype(jnp.bfloat16)

    def project(g, low):
        return jnp.dot(normed[pl.ds(low, hrow)], wg[g], preferred_element_type=jnp.float32)

    edge = 16
    has_next, has_prev = block_of + 1 < nsp, block_of >= 1
    next_at = at(z + c, y, x, 1 - c)
    prev_at = at(z + c - 1, y, x, 1 - c)

    def halo_copy(way, what):
        cols = pl.ds(0, gw) if what == 0 else pl.ds(gw, pn)
        count = WINDOW if what == 0 else edge
        if way == 0:
            src, dst = WINDOW + rows - count, WINDOW - count
        else:
            src, dst = WINDOW, WINDOW + rows
        return remote(
            ext.at[pl.ds(src, count), cols],
            ext.at[pl.ds(dst, count), cols],
            h_send.at[way, what],
            h_recv.at[way, what],
            next_at if way == 0 else prev_at,
        )

    def halo_send(what, done=False):
        for way, ok in ((0, has_next), (1, has_prev)):

            @pl.when(ok)
            def _():
                if done:
                    halo_copy(way, what).wait_send()
                else:
                    halo_copy(way, what).start()

    def halo_wait(what, near):
        for way, ok in ((0, has_prev), (1, has_next)):
            inside_chip = c == 1 if way == 0 else c == 0

            @pl.when(ok & (inside_chip if near else jnp.logical_not(inside_chip)))
            def _():
                halo_copy(way, what).wait_recv()

    gathered(0)
    for low in range(0, rows, hrow):
        pair = project(0, low)
        into = pl.ds(WINDOW + low, hrow)
        for col in range(0, kn, 128):
            ext[into, col : col + 128] = turn(pair[:, col : col + 128], low, 1.0)
        ext[into, kn:gw] = pair[:, kn:].astype(jnp.bfloat16)
    halo_send(0)

    stage(nz + 2, nz + 4, middle)
    stage(nz, nz + 2, outer)
    gathered(1)
    for low in range(0, rows, hrow):
        ext[pl.ds(WINDOW + low, hrow), gw : gw + pn] = project(1, low).astype(jnp.bfloat16)
    halo_send(1)
    stage(nz + 4, nz + 2 * groups, middle)
    behind = (z, nz - 1 - z)

    def own_out(ok, wait, ways, crowded):
        @pl.when(ok)
        def _():
            for p in range(groups, pieces):
                if wait:
                    load_wait(p)
                    w_copy(p, block_of, 2).start()
                for way in ways:

                    @pl.when(onward[way] & ((behind[way] > 1) == crowded))
                    def _():
                        w_copy(p, block_of, way).start()

    own_out(outer, True, (0, 1), False)
    span = 3 * WINDOW
    row_at = lax.broadcasted_iota(jnp.int32, (WINDOW, span), 0)
    key_at = lax.broadcasted_iota(jnp.int32, (WINDOW, span), 1)
    apart = key_at - row_at
    key_down = lax.broadcasted_iota(jnp.int32, (WINDOW, WINDOW), 0)
    query_over = lax.broadcasted_iota(jnp.int32, (WINDOW, WINDOW), 1)
    half_width = jnp.left_shift(jnp.int32(1), group_of)
    n_blocks = rows // WINDOW

    def inside_of(i):
        first = block_of * rows + (i - 1) * WINDOW
        return (key_at + first >= 0) & (key_at + first < seq_total)

    def attend(kv, i):
        q_at = pl.ds(pl.multiple_of(i * WINDOW, WINDOW), WINDOW)
        window = pl.ds(pl.multiple_of(i * WINDOW, WINDOW), span)
        first = block_of * rows + (i - 1) * WINDOW
        low = (key_down >= query_over) & (first >= 0)
        high = (key_down <= query_over) & (first + 2 * WINDOW < seq_total)
        keys = ext[window, kv * HD : (kv + 1) * HD]
        values = ext[window, kn + kv * HD : kn + (kv + 1) * HD].T
        weights, shares = [], []
        for g in range(grp):
            head = kv * grp + g
            query = qrot[q_at, head * HD : (head + 1) * HD]
            score = lax.dot_general(
                keys, query, (((1,), (1,)), ((), ())), preferred_element_type=jnp.float32
            )
            score = jnp.concatenate(
                [
                    jnp.where(low, score[:WINDOW], neg_fill),
                    score[WINDOW : 2 * WINDOW],
                    jnp.where(high, score[2 * WINDOW :], neg_fill),
                ],
                0,
            )
            sink = sinkb[head : head + 1, :]
            top = jnp.maximum(jnp.max(score, 0, keepdims=True), sink)
            exps = jnp.exp(score - top)
            total = jnp.sum(exps, 0, keepdims=True) + jnp.exp(sink - top)
            log_own[head : head + 1, q_at] = top + jnp.log(total)
            weights.append(exps.astype(jnp.bfloat16))
            shares.append(1.0 / total)
        out = jnp.dot(values, jnp.concatenate(weights, 1), preferred_element_type=jnp.float32)
        outs = [out[:, g * WINDOW : (g + 1) * WINDOW] * shares[g] for g in range(grp)]
        col = pn + kv * grp * HD
        act[q_at, col : col + grp * HD] = jnp.concatenate(outs, 0).T.astype(jnp.bfloat16)

    late = jnp.where(c == 0, 0, n_blocks - 1)
    early = n_blocks - 1 - late

    def attend_early(kv):
        for i in range(1, n_blocks - 1):
            attend(kv, i)
        attend(kv, early)

    def queries(kv, g):
        for low in range(0, rows, hrow):
            both = project(g, low)
            for col in range(0, gw, 128):
                at_col = kv * gw + col
                qrot[pl.ds(low, hrow), at_col : at_col + 128] = turn(
                    both[:, col : col + 128], low, HD ** -0.5
                )

    @pl.when(crossed)
    def _():
        remote(sink_own, sinkb, m_send.at[1], m_recv.at[1], partner).wait_recv()

    def pool(i):
        q_at = pl.ds(pl.multiple_of(i * WINDOW, WINDOW), WINDOW)
        window = pl.ds(pl.multiple_of(i * WINDOW, WINDOW), span)
        own_at = pl.ds(pl.multiple_of((i + 1) * WINDOW, WINDOW), WINDOW)
        band = inside_of(i) & (apart >= WINDOW - half_width) & (apart < WINDOW + half_width)
        band_f = band.astype(jnp.float32)
        counted = jnp.sum(band_f, -1, keepdims=True)
        summed = jnp.dot(
            band_f.astype(jnp.bfloat16),
            ext[window, gw : gw + pn],
            preferred_element_type=jnp.float32,
        )
        own_pool = ext[own_at, gw : gw + pn]
        pooled = (summed / counted - own_pool.astype(jnp.float32)).astype(jnp.bfloat16)
        act[q_at, 0:pn] = jnp.dot(
            pooled, mixb[...], preferred_element_type=jnp.float32
        ).astype(jnp.bfloat16)

    halo_wait(1, True)

    @pl.when(straight)
    def _():
        mix_local.wait()

    @pl.when(crossed)
    def _():
        mix_swap.wait_recv()

    for i in range(1, n_blocks - 1):
        pool(i)
    pool(early)

    stage(nz + 2, nz + 4, outer)
    gathered(2)
    queries(0, 2)
    halo_wait(0, True)
    own_out(middle, True, (0, 1), False)
    attend_early(0)
    own_out(middle, False, (0, 1), True)
    stage(nz + 4, nz + 2 * groups, outer)
    halo_wait(0, False)
    attend(0, late)
    halo_wait(1, False)
    pool(late)

    x_first = ((0, HALVES - 1), (2, 0))

    def side_of(block):
        return block // per_owner // CORES

    def r1_copy(block, h, rh, turned):
        take = pl.ds(rh * hrow, hrow)
        return remote(
            part.at[h, block, take],
            rs1.at[h, block, take],
            r1_send.at[h, int(turned)],
            r1_recv.at[h, block, rh],
            at(z, y, 1 - x, c) if turned else at(z, 1 - y, x, c),
        )

    def r2_copy(block, h, rh, turned):
        take = pl.ds(rh * hrow, hrow)
        owner = block // per_owner
        slot = block % per_owner
        side = jnp.where(straight if turned else side_of(block) == x, 0, 1)
        return remote(
            tot.at[h, block, take],
            fin.at[side, h, slot, take],
            r2_send.at[h, int(turned)],
            r2_recv.at[side],
            (z * NY + c, owner),
        )

    def each_block(d, lead, body):
        parity = y if lead == 0 else 1 - y
        for way in range(1 if d == 0 else 2):
            source = z + (2 * way - 1) * d

            @pl.when((source >= 0) & (source < nz))
            def _():
                body(source * NY + parity)

    def compute(d, h, lead, halves=(0, 1)):
        def body(block):
            if halves[0] == 0:

                @pl.when(crossed if lead == 0 else straight)
                def _():
                    w_copy(groups + h, block, 2).wait_recv()

            take = pl.ds(halves[0] * hrow, len(halves) * hrow)
            part[h, block, take] = jnp.dot(
                act[take], wo[block, h], preferred_element_type=jnp.float32
            ).astype(jnp.bfloat16)

            turned = (d, h) in x_first

            @pl.when(side_of(block) != x if turned else crossed)
            def _():
                for rh in halves:
                    r1_copy(block, h, rh, turned).start()

        each_block(d, lead, body)

    def join(d, h):
        turned = (d, h) in x_first

        def meet(block):
            for rh in range(2):
                take = pl.ds(rh * hrow, hrow)
                r1_copy(block, h, rh, turned).wait_recv()
                tot[h, block, take] = (
                    part[h, block, take].astype(jnp.float32)
                    + rs1[h, block, take].astype(jnp.float32)
                ).astype(jnp.bfloat16)

                @pl.when(crossed | (block // per_owner != tp))
                def _():
                    r2_copy(block, h, rh, turned).start()

        def body(block):
            @pl.when(side_of(block) == x if turned else straight)
            def _():
                meet(block)

        for lead in range(2):
            each_block(d, lead, body)

    gathered(3)
    queries(1, 3)
    log_swap = remote(log_own, log_in, m_send.at[2], m_recv.at[2], partner)

    for rh in range(2):
        for i in range(rh * n_blocks // 2, (rh + 1) * n_blocks // 2):
            attend(1, i)
        for h in range(HALVES):
            for lead in range(2):
                compute(0, h, lead, (rh,))

    @pl.when(crossed)
    def _():
        log_swap.start()

    def pass_on(d, h, ok):
        @pl.when(ok)
        def _():
            relay(d, groups + h)

    order = [(d, h) for d in range(nz) for h in range(HALVES)]

    def advance(n):
        d, h = order[n]
        compute(d, h, 0)
        pass_on(d, h, outer & crossed)
        if n + 1 < len(order):
            pass_on(*order[n + 1], outer & straight)
        compute(d, h, 1)

    for h in range(HALVES):
        pass_on(1, h, middle)
    for n in range(HALVES, len(order)):
        if n == HALVES:
            pass_on(*order[n], outer & straight)
        advance(n)
        if n == 2 * HALVES - 1:
            join(*order[0])
            for far in range(2, nz):
                for h in range(HALVES):
                    pass_on(far, h, middle)
        for ready in {4: (1, 2, 3), 6: (4, 5)}.get(n, ()):
            join(*order[ready])
    for ready in (6, 7):
        join(*order[ready])

    @pl.when(straight)
    def _():
        log_ref[...] = log_own[...]

    @pl.when(crossed)
    def _():
        log_swap.wait_recv()
        log_ref[...] = log_in[...]

    arrived(fin.at[1], r2_recv.at[1])

    @pl.when(crossed)
    def _():
        arrived(fin.at[0], r2_recv.at[0])

    for slot in range(per_owner):
        for h in range(HALVES):
            low = (slot * HALVES + h) * ohalf
            far = fin[1, h, slot].astype(jnp.float32)

            @pl.when(straight)
            def _():
                near = tot[h, tp * per_owner + slot].astype(jnp.float32)
                mixed_ref[:, low : low + ohalf] = (near + far).astype(jnp.bfloat16)

            @pl.when(crossed)
            def _():
                near = fin[0, h, slot].astype(jnp.float32)
                mixed_ref[:, low : low + ohalf] = (near + far).astype(jnp.bfloat16)

    def all_sent(way, count):
        departed(wg.at[pl.ds(0, groups), pl.ds(0, count * brow)], w_send.at[way, 0])
        departed(wo.at[pl.ds(0, count)], w_send.at[way, 1])

    all_sent(2, nz)
    for count in range(1, nz):
        for way, passed in ((0, z + 1), (1, nz - z)):

            @pl.when(onward[way] & (passed == count))
            def _():
                all_sent(way, count)

    halo_send(0, done=True)
    halo_send(1, done=True)

    @pl.when(straight)
    def _():
        departed(xg.at[pl.ds(0, 2)], x_send.at[0])
        departed(xg.at[pl.ds(0, CORES), spans[0]], x_send.at[1])

    @pl.when(crossed)
    def _():
        departed(xg.at[pl.ds(0, 3)], x_send.at[0])
        departed(xg.at[pl.ds(0, CORES), spans[1]], x_send.at[1])
        departed(wg.at[pl.ds(0, groups), pl.ds(0, brow)], load_send.at[0])
        departed(wo.at[0], load_send.at[1])
        mix_swap.wait_send()
        sink_swap.wait_send()
        log_swap.wait_send()

    for d, h in x_first:
        across = z if d == 0 else (z + d) % nz
        owner = across * NY // per_owner
        facing = owner // CORES == x
        plain = nsp - NY

        def gone(ok, source, count, sem):
            @pl.when(ok)
            def _():
                departed(source.at[h, pl.ds(0, count)], sem)

        gone(jnp.logical_not(facing), part, NY, r1_send.at[h, 1])
        gone(facing & (crossed | (owner != tp)), tot, NY, r2_send.at[h, 1])
        gone(crossed, part, plain, r1_send.at[h, 0])
        gone(straight & (owner == tp), tot, plain, r2_send.at[h, 0])
        gone(straight & (owner != tp), tot, plain - per_owner, r2_send.at[h, 0])


def place_kernel(mixed_ref, log_ref, mixed_out, log_out, sems):
    copies = [
        pltpu.make_async_copy(mixed_ref, mixed_out, sems.at[0]),
        pltpu.make_async_copy(log_ref, log_out, sems.at[1]),
    ]
    for copy in copies:
        copy.start()
    for copy in copies:
        copy.wait()


def fused(
    nz,
    ntp,
    tokens,
    norm_gain,
    query_weight,
    key_weight,
    value_weight,
    pool_in_weight,
    pool_mix_weight,
    sink_logit,
    out_pool_weight,
    out_attn_weight,
):
    rows, width = tokens.shape
    nsp = nz * NY
    dim = width * ntp
    qn, kn, pn = query_weight.shape[1], key_weight.shape[1], pool_in_weight.shape[1]
    fan = out_pool_weight.shape[0] + out_attn_weight.shape[0]
    ohalf = out_pool_weight.shape[1] // HALVES
    heads = sink_logit.shape[0]
    gw = 2 * kn
    groups = (qn + 2 * kn + pn) // gw
    pieces = groups + HALVES
    hbm = pl.BlockSpec(memory_space=pl.ANY)
    vmem = pl.BlockSpec(memory_space=pltpu.VMEM)
    dma = pltpu.SemaphoreType.DMA
    bf16 = jnp.bfloat16
    f32 = jnp.float32
    per_owner = nsp // ntp
    outs = (
        jax.ShapeDtypeStruct((rows, width), bf16),
        jax.ShapeDtypeStruct((heads, rows), f32),
    )
    mixed, logs = pl.pallas_call(
        functools.partial(layer_kernel, nz, ntp),
        out_shape=outs,
        in_specs=[hbm] * 10,
        out_specs=(vmem, vmem),
        scratch_shapes=[
            pltpu.VMEM((ntp, rows, width), bf16),
            pltpu.VMEM((rows, dim), bf16),
            pltpu.VMEM((groups, dim, gw), bf16),
            pltpu.VMEM((nsp, HALVES, fan, ohalf), bf16),
            pltpu.VMEM((rows, qn), bf16),
            pltpu.VMEM((rows + 2 * WINDOW, gw + pn), bf16),
            pltpu.VMEM((rows, fan), bf16),
            pltpu.VMEM((HALVES, nsp, rows, ohalf), bf16),
            pltpu.VMEM((HALVES, nsp, rows, ohalf), bf16),
            pltpu.VMEM((HALVES, nsp, rows, ohalf), bf16),
            pltpu.VMEM((2, HALVES, per_owner, rows, ohalf), bf16),
            pltpu.VMEM((rows, 128), f32),
            pltpu.VMEM((rows, 128), f32),
            pltpu.VMEM((pn, pn), bf16),
            pltpu.VMEM((1, dim), f32),
            pltpu.SMEM((heads,), f32),
            pltpu.VMEM((heads, 128), f32),
            pltpu.VMEM((heads, 128), f32),
            pltpu.VMEM((heads, rows), f32),
            pltpu.VMEM((heads, rows), f32),
            dma((2,)),
            dma((pieces,)),
            dma((3, 2)),
            dma((pieces, nz)),
            dma((groups,)),
            dma((HALVES, nz)),
            dma,
            dma((2,)),
            dma((ntp, 2)),
            dma((2,)),
            dma((3,)),
            dma((3,)),
            dma((2, 2)),
            dma((2, 2)),
            dma((HALVES, 2)),
            dma((HALVES, nsp, 2)),
            dma((HALVES, 2)),
            dma((2,)),
        ],
        compiler_params=pltpu.CompilerParams(
            collective_id=0, has_side_effects=True, vmem_limit_bytes=56 << 20
        ),
    )(
        tokens,
        norm_gain[None, :],
        query_weight,
        key_weight,
        value_weight,
        pool_in_weight,
        pool_mix_weight,
        sink_logit,
        out_pool_weight,
        out_attn_weight,
    )
    return pl.pallas_call(
        place_kernel,
        out_shape=outs,
        in_specs=[vmem, vmem],
        out_specs=(hbm, hbm),
        scratch_shapes=[dma((2,))],
    )(mixed, logs)


def choose(mesh):
    nsp, ntp = mesh.shape["sp"], mesh.shape["tp"]

    def body(*args):
        rows = args[0].shape[0]
        qn, kn, pn = args[2].shape[1], args[3].shape[1], args[5].shape[1]
        columns = args[8].shape[1]
        grid = nsp == 4 * NY and ntp == NX * CORES and nsp == NY * ntp
        cuts = columns % (HALVES * 128) == 0 and rows % (4 * WINDOW) == 0
        even = kn == 2 * HD and kn % 128 == 0 and qn == 4 * kn and pn == 2 * kn
        if grid and cuts and even:
            return fused(nsp // NY, ntp, *args)
        return local(*args)

    return body


def solution(mesh):
    return jax.shard_map(
        choose(mesh),
        mesh=mesh,
        in_specs=(
            P("sp", "tp"),
            P(),
            P("sp", "tp"),
            P("sp", "tp"),
            P("sp", "tp"),
            P("sp", "tp"),
            P("tp", None, None),
            P("tp"),
            P("tp", "sp"),
            P("tp", "sp"),
        ),
        out_specs=(P("sp", "tp"), P("tp", "sp")),
        check_vma=False,
    )
```

```python
import functools
import math

import jax
import jax.numpy as jnp
from jax import lax
from jax.experimental import pallas as pl
from jax.experimental.pallas import tpu as pltpu
from jax.sharding import PartitionSpec as P

HD = 64
WINDOW = 128
GRID_W = 64


norm_eps = 1e-06
rope_base = 10000.0
pool_reach = 8
neg_fill = -1e30


def with_halo(cells, sides, width):
    for axis, dim in sides:
        count = lax.axis_size(axis)
        ends = count - 1
        head = lax.slice_in_dim(cells, 0, width, axis=dim)
        tail = lax.slice_in_dim(cells, cells.shape[dim] - width, cells.shape[dim], axis=dim)
        cells = jnp.concatenate(
            [
                lax.ppermute(tail, axis, [(i, (i + 1) % count) for i in range(ends)]),
                cells,
                lax.ppermute(head, axis, [((i + 1) % count, i) for i in range(ends)]),
            ],
            axis=dim,
        )
    return cells


def rope_tables(positions, head_dim):
    n_freq = head_dim // 4
    freqs = rope_base ** (-jnp.arange(n_freq, dtype=jnp.float32) / n_freq)
    rows = (positions // GRID_W).astype(jnp.float32)
    columns = (positions % GRID_W).astype(jnp.float32)
    row_angle = rows[:, None] * freqs[None, :]
    col_angle = columns[:, None] * freqs[None, :]
    return (jnp.cos(row_angle), jnp.sin(row_angle), jnp.cos(col_angle), jnp.sin(col_angle))


def rotate_half(values, cosine, sine):
    middle = values.shape[-1] // 2
    first = values[..., :middle]
    second = values[..., middle:]
    return jnp.concatenate([first * cosine - second * sine, second * cosine + first * sine], -1)


def rotate_heads(values, tables, head_dim):
    rows_count = values.shape[0]
    shaped = values.astype(jnp.float32).reshape(rows_count, -1, head_dim)
    cos_r, sin_r, cos_c, sin_c = [table[:, None, :] for table in tables]
    split = head_dim // 2
    turned = jnp.concatenate(
        [
            rotate_half(shaped[..., :split], cos_r, sin_r),
            rotate_half(shaped[..., split:], cos_c, sin_c),
        ],
        -1,
    )
    return turned.reshape(rows_count, -1).astype(jnp.bfloat16)


def pool_group(extended, own, positions, half_width, seq_total):
    rows_count = own.shape[0]
    summed = jnp.zeros(own.shape, jnp.float32)
    counted = jnp.zeros((rows_count,), jnp.float32)
    for shift_by in range(-pool_reach, pool_reach):
        source = positions + shift_by
        inside = (
            (shift_by >= -half_width)
            & (shift_by < half_width)
            & (source >= 0)
            & (source < seq_total)
        )
        window_rows = extended[pool_reach + shift_by : pool_reach + shift_by + rows_count].astype(
            jnp.float32
        )
        summed = summed + jnp.where(inside[:, None], window_rows, 0.0)
        counted = counted + inside.astype(jnp.float32)
    return (summed / counted[:, None] - own.astype(jnp.float32)).astype(jnp.bfloat16)


def attend_block(queries, keys, values, sink, query_pos, key_pos, seq_total):
    scores = jnp.einsum(
        "qhgd,khd->hgqk", queries, keys, preferred_element_type=jnp.float32
    ) * HD ** (-0.5)
    valid = (
        (jnp.abs(query_pos[:, None] - key_pos[None, :]) <= WINDOW)
        & (key_pos >= 0)[None, :]
        & (key_pos < seq_total)[None, :]
    )
    scores = jnp.where(valid, scores, neg_fill)
    row_top = jnp.maximum(jnp.max(scores, -1), sink[:, :, None])
    exps = jnp.exp(scores - row_top[..., None])
    row_total = jnp.sum(exps, -1) + jnp.exp(sink[:, :, None] - row_top)
    weights = (exps / row_total[..., None]).astype(jnp.bfloat16)
    attended = jnp.einsum("hgqk,khd->qhgd", weights, values, preferred_element_type=jnp.float32)
    return (attended.astype(jnp.bfloat16), row_top + jnp.log(row_total))


def fetch_outputs(out_pool_weight, out_attn_weight):
    return (
        lax.all_gather(out_pool_weight, "sp", axis=1, tiled=True),
        lax.all_gather(out_attn_weight, "sp", axis=1, tiled=True),
    )


def local(
    tokens,
    norm_gain,
    query_weight,
    key_weight,
    value_weight,
    pool_in_weight,
    pool_mix_weight,
    sink_logit,
    out_pool_weight,
    out_attn_weight,
):
    whole = lax.all_gather(tokens, "tp", axis=1, tiled=True)
    wide = whole.astype(jnp.float32)
    normed = (
        wide * lax.rsqrt(jnp.mean(wide * wide, -1, keepdims=True) + norm_eps) * norm_gain
    ).astype(jnp.bfloat16)
    tok_rows = normed.shape[0]
    seq_total = tok_rows * lax.axis_size("sp")
    offset = lax.axis_index("sp") * tok_rows
    weights_in = (query_weight, key_weight, value_weight, pool_in_weight)
    pieces = (
        lax.all_gather(weights_in[0], "sp", axis=0, tiled=True),
        lax.all_gather(weights_in[1], "sp", axis=0, tiled=True),
        lax.all_gather(weights_in[2], "sp", axis=0, tiled=True),
        lax.all_gather(weights_in[3], "sp", axis=0, tiled=True),
    )
    sums = tuple((jnp.dot(normed, piece, preferred_element_type=jnp.float32) for piece in pieces))
    query, key, value, pool_input = [total.astype(jnp.bfloat16) for total in sums]
    positions = offset + jnp.arange(tok_rows, dtype=jnp.int32)
    tables = rope_tables(positions, HD)
    rot_query = rotate_heads(query, tables, HD)
    rot_key = rotate_heads(key, tables, HD)
    key_width = rot_key.shape[1]
    pool_ext = with_halo(pool_input, (("sp", 0),), pool_reach)
    pair_ext = with_halo(jnp.concatenate([rot_key, value], 1), (("sp", 0),), WINDOW)
    key_ext = pair_ext[:, :key_width]
    value_ext = pair_ext[:, key_width:]
    half_width = jnp.left_shift(jnp.int32(1), lax.axis_index("tp"))
    pooled = pool_group(pool_ext, pool_input, positions, half_width, seq_total)
    pool_out = jnp.dot(pooled, pool_mix_weight[0], preferred_element_type=jnp.float32).astype(
        jnp.bfloat16
    )
    heads_local = rot_query.shape[1] // HD
    kv_local = key_width // HD
    grp = heads_local // kv_local
    query_heads = rot_query.reshape(tok_rows, kv_local, grp, HD)
    key_heads = key_ext.reshape(-1, kv_local, HD)
    value_heads = value_ext.reshape(-1, kv_local, HD)
    sink = sink_logit.reshape(kv_local, grp)
    block_rows = min(tok_rows, 256)
    attended_parts = []
    log_parts = []
    for block_index in range(tok_rows // block_rows):
        start = block_index * block_rows
        query_pos = offset + start + jnp.arange(block_rows, dtype=jnp.int32)
        key_pos = offset + start - WINDOW + jnp.arange(block_rows + 2 * WINDOW, dtype=jnp.int32)
        attended_block, log_block = attend_block(
            query_heads[start : start + block_rows],
            key_heads[start : start + block_rows + 2 * WINDOW],
            value_heads[start : start + block_rows + 2 * WINDOW],
            sink,
            query_pos,
            key_pos,
            seq_total,
        )
        attended_parts.append(attended_block.reshape(block_rows, heads_local * HD))
        log_parts.append(log_block.reshape(heads_local, block_rows))
    attended = jnp.concatenate(attended_parts, 0)
    log_weight = jnp.concatenate(log_parts, 1)
    out_pool_full, out_attn_full = fetch_outputs(out_pool_weight, out_attn_weight)
    term = jnp.dot(pool_out, out_pool_full, preferred_element_type=jnp.float32)
    term = term + jnp.dot(attended, out_attn_full, preferred_element_type=jnp.float32)
    mixed = lax.psum_scatter(term.astype(jnp.bfloat16), "tp", scatter_dimension=1, tiled=True)
    return (mixed, log_weight)


NY = 2
NX = 2
CORES = 2
HALVES = 2
MESH = pl.DeviceIdType.MESH


def layer_kernel(
    nz,
    ntp,
    tok_ref,
    gain_ref,
    qw_ref,
    kw_ref,
    vw_ref,
    pw_ref,
    mix_ref,
    sink_ref,
    ow_ref,
    aw_ref,
    mixed_ref,
    log_ref,
    xg,
    normed,
    wg,
    wo,
    qrot,
    ext,
    act,
    part,
    rs1,
    tot,
    fin,
    cos_ref,
    sin_ref,
    mixb,
    gain,
    sinks,
    sink_own,
    sinkb,
    log_own,
    log_in,
    load_send,
    load_recv,
    w_send,
    w_recv,
    s_recv,
    o_recv,
    x_loc,
    x_send,
    x_recv,
    g_sem,
    m_send,
    m_recv,
    h_send,
    h_recv,
    r1_send,
    r1_recv,
    r2_send,
    r2_recv,
):
    sp, tp = lax.axis_index("sp"), lax.axis_index("tp")
    z, y = sp // NY, sp % NY
    x, c = tp // CORES, tp % CORES
    nsp = nz * NY
    block_of = z * NY + c
    group_of = x * CORES + y
    straight = c == y
    crossed = c != y
    rows, width = tok_ref.shape
    brow = qw_ref.shape[0]
    qn, kn, pn = qw_ref.shape[1], kw_ref.shape[1], pw_ref.shape[1]
    heads, kv_local = qn // HD, kn // HD
    grp = heads // kv_local
    gw = 2 * kn
    groups = wg.shape[0]
    pool_rows = ow_ref.shape[0]
    ohalf = wo.shape[3]
    seq_total = rows * nsp
    per_owner = nsp // ntp
    pieces = groups + HALVES

    def at(zz, yy, xx, cc):
        return (zz * NY + yy, xx * CORES + cc)

    def remote(src, dst, send, recv, target):
        return pltpu.make_async_remote_copy(
            src_ref=src,
            dst_ref=dst,
            send_sem=send,
            recv_sem=recv,
            device_id=target,
            device_id_type=MESH,
        )

    sibling = at(z, y, x, 1 - c)
    partner = at(z, 1 - y, x, 1 - c)

    def shard_rows(block):
        return pl.ds(pl.multiple_of(block * brow, brow), brow)

    def load_parts(p, block):
        if p == 0:
            return [
                (kw_ref, wg.at[0, shard_rows(block), pl.ds(0, kn)]),
                (vw_ref, wg.at[0, shard_rows(block), pl.ds(kn, kn)]),
            ]
        if p == 1:
            return [(pw_ref, wg.at[1, shard_rows(block)])]
        if p < groups:
            return [(qw_ref.at[:, pl.ds((p - 2) * gw, gw)], wg.at[p, shard_rows(block)])]
        h = p - groups
        cols = pl.ds(h * ohalf, ohalf)
        return [
            (ow_ref.at[:, cols], wo.at[block, h, pl.ds(0, pool_rows)]),
            (aw_ref.at[:, cols], wo.at[block, h, pl.ds(pool_rows, wo.shape[2] - pool_rows)]),
        ]

    def load_local(p):
        return [
            pltpu.make_async_copy(a, b, load_recv.at[p]) for a, b in load_parts(p, sp)
        ]

    def load_swap(p):
        return [
            remote(a, b, load_send.at[p // groups], load_recv.at[p], partner)
            for a, b in load_parts(p, sp)
        ]

    def piece_of(p, block):
        return wg.at[p, shard_rows(block)] if p < groups else wo.at[block, p - groups]

    def arrived(ref, sem):
        remote(ref, ref, load_send.at[0], sem, sibling).wait_recv()

    def departed(ref, sem):
        remote(ref, ref, sem, load_recv.at[0], sibling).wait_send()

    def load_wait(p):
        arrived(piece_of(p, block_of), load_recv.at[p])

    onward = (z + 1 < nz, z >= 1)
    middle = onward[0] & onward[1]
    outer = jnp.logical_not(middle)

    def w_copy(p, block, way):
        ref = piece_of(p, block)
        target = (at(z + 1, y, x, c), at(z - 1, y, x, c), sibling)[way]
        if way < 2:
            recv = w_recv.at[p, block // NY]
        elif p < groups:
            recv = s_recv.at[p]
        else:
            recv = o_recv.at[p - groups, block // NY]
        return remote(ref, ref, w_send.at[way, p // groups], recv, target)

    def send_own(p, ways):
        for way in ways:
            if way == 2:
                w_copy(p, block_of, 2).start()
            else:

                @pl.when(onward[way])
                def _():
                    w_copy(p, block_of, way).start()

    def relay(d, p):
        for way in range(2):
            source = (z - d, z + d)[way]
            block = source * NY + c

            @pl.when((source >= 0) & (source < nz))
            def _():
                w_copy(p, block, way).wait_recv()

                @pl.when(onward[way])
                def _():
                    w_copy(p, block, way).start()

                w_copy(p, block, 2).start()

    def stage(low, high, ok=None):
        if ok is not None:

            @pl.when(ok)
            def _():
                stage(low, high)

            return
        for turn_at in range(low, high):
            for p in range(groups):
                for role, when in ((straight, max(p - 1, 0)), (crossed, p)):
                    if when == turn_at:

                        @pl.when(role)
                        def _():
                            load_wait(p)
                            send_own(p, (0, 1, 2))

            for d in range(1, nz):
                for p in range(groups):
                    if turn_at == 2 * p + d:
                        relay(d, p)

    def gathered(p):
        arrived(wg.at[p, pl.ds(0, nz * brow)], s_recv.at[p])

    cut = rows // 4
    spans = (pl.ds(0, cut), pl.ds(cut, rows - cut))

    def token_copy(kind, r):
        target = (at(z, y, x, y), at(z, y, 1 - x, y), at(z, 1 - y, x, y))[kind]
        return remote(
            tok_ref.at[spans[r]], xg.at[tp, spans[r]], x_send.at[0], x_recv.at[tp, r], target
        )

    token_local = pltpu.make_async_copy(tok_ref, xg.at[tp], x_loc)

    def token_relay(k, r):
        slot = ((1 - x) if r == 0 else x) * CORES + k
        target = at(z, 1 - y, x, c) if r == 0 else at(z, y, 1 - x, c)
        ref = xg.at[slot, spans[r]]
        return remote(ref, ref, x_send.at[1], x_recv.at[slot, r], target)

    def token_wait(slot, r):
        arrived(xg.at[slot, spans[r]], x_recv.at[slot, r])

    mix_local = pltpu.make_async_copy(mix_ref.at[0], mixb, m_recv.at[0])
    mix_swap = remote(mix_ref.at[0], mixb, m_send.at[0], m_recv.at[0], partner)
    sink_swap = remote(sink_own, sinkb, m_send.at[1], m_recv.at[1], partner)

    gain_load = pltpu.make_async_copy(gain_ref, gain, g_sem.at[0])
    sink_load = pltpu.make_async_copy(sink_ref, sinks, g_sem.at[1])
    sink_load.start()
    gain_load.start()

    @pl.when(straight)
    def _():
        for p in range(groups):
            for copy in load_local(p):
                copy.start()
        token_local.start()

    barrier = pltpu.get_barrier_semaphore()
    met = jnp.int32(0)
    for flip in range(1, NY * NX * CORES):
        fy, fx, fc = flip // 4, (flip // 2) % 2, flip % 2
        pl.semaphore_signal(
            barrier,
            inc=1,
            device_id=at(
                z,
                1 - y if fy else y,
                1 - x if fx else x,
                1 - c if fc else c,
            ),
            device_id_type=MESH,
        )
        met = met + 1
    for ok, zz in ((onward[0], z + 1), (onward[1], z - 1)):
        met = met + CORES * ok.astype(jnp.int32)

        @pl.when(ok)
        def _():
            for cc in range(CORES):
                pl.semaphore_signal(
                    barrier, inc=1, device_id=at(zz, y, x, cc), device_id_type=MESH
                )

    ext[...] = jnp.zeros_like(ext)
    sink_load.wait()
    for head in range(heads):
        sink_own[head : head + 1, :] = jnp.full((1, 128), sinks[head], jnp.float32)

    @pl.when(straight)
    def _():
        sinkb[...] = sink_own[...]

    pl.semaphore_wait(barrier, met)

    @pl.when(straight)
    def _():
        for kind in (1, 2):
            for r in range(2):
                token_copy(kind, r if kind == 1 else 1 - r).start()
        mix_local.start()
        for p in range(groups, pieces):
            for copy in load_local(p):
                copy.start()

    @pl.when(crossed)
    def _():
        for r in range(2):
            token_copy(1, r).start()
            token_copy(0, r).start()
        for p in range(groups):
            for copy in load_swap(p):
                copy.start()
        token_copy(2, 1).start()
        token_copy(2, 0).start()
        sink_swap.start()
        mix_swap.start()
        for p in range(groups, pieces):
            for copy in load_swap(p):
                copy.start()

    stage(0, 1)

    half = HD // 4
    lane = lax.broadcasted_iota(jnp.int32, (rows, 128), 1)
    is_first = (lane % (2 * half)) < half
    position = block_of * rows + lax.broadcasted_iota(jnp.int32, (rows, 128), 0)
    place = jnp.where((lane % HD) < 2 * half, position // GRID_W, position % GRID_W)
    freqs = jnp.exp((lane % half).astype(jnp.float32) * (-math.log(rope_base) / half))
    angle = place.astype(jnp.float32) * freqs
    cos_ref[...] = jnp.cos(angle)
    sine = jnp.sin(angle)
    sin_ref[...] = jnp.where(is_first, -sine, sine)

    stage(1, 2)

    @pl.when(straight)
    def _():
        for k in range(CORES):
            token_relay(k, 0).wait_recv()
            token_relay(k, 0).start()

    @pl.when(crossed)
    def _():
        token_relay(c, 1).wait_recv()
        token_relay(c, 1).start()

    stage(2, nz)

    @pl.when(crossed)
    def _():
        token_relay(1 - c, 1).wait_recv()
        token_relay(1 - c, 1).start()

    stage(nz, nz + 2, middle)

    @pl.when(straight)
    def _():
        token_local.wait()
        for r in range(2):
            token_wait(x * CORES + (1 - c), r)
        for k in range(CORES):
            token_wait((1 - x) * CORES + k, 1)

    @pl.when(crossed)
    def _():
        for k in range(CORES):
            token_wait(x * CORES + k, 0)
            for r in range(2):
                token_wait((1 - x) * CORES + k, r)

    gain_load.wait()
    norm_rows = 128

    @pl.loop(0, rows // norm_rows)
    def _(i):
        take = pl.ds(pl.multiple_of(i * norm_rows, norm_rows), norm_rows)
        pieces_in = [xg[t, take, :].astype(jnp.float32) for t in range(ntp)]
        total = sum(jnp.sum(piece * piece, -1, keepdims=True) for piece in pieces_in)
        scale = lax.rsqrt(total / (width * ntp) + norm_eps)
        for t in range(ntp):
            cols = pl.ds(t * width, width)
            normed[take, cols] = (pieces_in[t] * scale * gain[:, cols]).astype(jnp.bfloat16)

    hrow = rows // 2
    lane_first = (lax.broadcasted_iota(jnp.int32, (hrow, 128), 1) % (2 * half)) < half

    def turn(values, low, factor):
        wide = values.astype(jnp.bfloat16).astype(jnp.float32)
        swapped = jnp.where(
            lane_first, pltpu.roll(wide, 128 - half, 1), pltpu.roll(wide, half, 1)
        )
        take = pl.ds(low, hrow)
        return ((wide * cos_ref[take] + swapped * sin_ref[take]) * factor).astype(jnp.bfloat16)

    def project(g, low):
        return jnp.dot(normed[pl.ds(low, hrow)], wg[g], preferred_element_type=jnp.float32)

    edge = 16
    has_next, has_prev = block_of + 1 < nsp, block_of >= 1
    next_at = at(z + c, y, x, 1 - c)
    prev_at = at(z + c - 1, y, x, 1 - c)

    def halo_copy(way, what):
        cols = pl.ds(0, gw) if what == 0 else pl.ds(gw, pn)
        count = WINDOW if what == 0 else edge
        if way == 0:
            src, dst = WINDOW + rows - count, WINDOW - count
        else:
            src, dst = WINDOW, WINDOW + rows
        return remote(
            ext.at[pl.ds(src, count), cols],
            ext.at[pl.ds(dst, count), cols],
            h_send.at[way, what],
            h_recv.at[way, what],
            next_at if way == 0 else prev_at,
        )

    def halo_send(what, done=False):
        for way, ok in ((0, has_next), (1, has_prev)):

            @pl.when(ok)
            def _():
                if done:
                    halo_copy(way, what).wait_send()
                else:
                    halo_copy(way, what).start()

    def halo_wait(what, near):
        for way, ok in ((0, has_prev), (1, has_next)):
            inside_chip = c == 1 if way == 0 else c == 0

            @pl.when(ok & (inside_chip if near else jnp.logical_not(inside_chip)))
            def _():
                halo_copy(way, what).wait_recv()

    gathered(0)
    for low in range(0, rows, hrow):
        pair = project(0, low)
        into = pl.ds(WINDOW + low, hrow)
        for col in range(0, kn, 128):
            ext[into, col : col + 128] = turn(pair[:, col : col + 128], low, 1.0)
        ext[into, kn:gw] = pair[:, kn:].astype(jnp.bfloat16)
    halo_send(0)

    stage(nz + 2, nz + 4, middle)
    stage(nz, nz + 2, outer)
    gathered(1)
    for low in range(0, rows, hrow):
        ext[pl.ds(WINDOW + low, hrow), gw : gw + pn] = project(1, low).astype(jnp.bfloat16)
    halo_send(1)
    stage(nz + 4, nz + 2 * groups, middle)
    behind = (z, nz - 1 - z)

    def own_out(ok, wait, ways, crowded):
        @pl.when(ok)
        def _():
            for p in range(groups, pieces):
                if wait:
                    load_wait(p)
                    w_copy(p, block_of, 2).start()
                for way in ways:

                    @pl.when(onward[way] & ((behind[way] > 1) == crowded))
                    def _():
                        w_copy(p, block_of, way).start()

    own_out(outer, True, (0, 1), False)
    span = 3 * WINDOW
    row_at = lax.broadcasted_iota(jnp.int32, (WINDOW, span), 0)
    key_at = lax.broadcasted_iota(jnp.int32, (WINDOW, span), 1)
    apart = key_at - row_at
    key_down = lax.broadcasted_iota(jnp.int32, (WINDOW, WINDOW), 0)
    query_over = lax.broadcasted_iota(jnp.int32, (WINDOW, WINDOW), 1)
    half_width = jnp.left_shift(jnp.int32(1), group_of)
    n_blocks = rows // WINDOW

    def inside_of(i):
        first = block_of * rows + (i - 1) * WINDOW
        return (key_at + first >= 0) & (key_at + first < seq_total)

    def attend(kv, i):
        q_at = pl.ds(pl.multiple_of(i * WINDOW, WINDOW), WINDOW)
        window = pl.ds(pl.multiple_of(i * WINDOW, WINDOW), span)
        first = block_of * rows + (i - 1) * WINDOW
        low = (key_down >= query_over) & (first >= 0)
        high = (key_down <= query_over) & (first + 2 * WINDOW < seq_total)
        keys = ext[window, kv * HD : (kv + 1) * HD]
        values = ext[window, kn + kv * HD : kn + (kv + 1) * HD].T
        weights, shares = [], []
        for g in range(grp):
            head = kv * grp + g
            query = qrot[q_at, head * HD : (head + 1) * HD]
            score = lax.dot_general(
                keys, query, (((1,), (1,)), ((), ())), preferred_element_type=jnp.float32
            )
            score = jnp.concatenate(
                [
                    jnp.where(low, score[:WINDOW], neg_fill),
                    score[WINDOW : 2 * WINDOW],
                    jnp.where(high, score[2 * WINDOW :], neg_fill),
                ],
                0,
            )
            sink = sinkb[head : head + 1, :]
            top = jnp.maximum(jnp.max(score, 0, keepdims=True), sink)
            exps = jnp.exp(score - top)
            total = jnp.sum(exps, 0, keepdims=True) + jnp.exp(sink - top)
            log_own[head : head + 1, q_at] = top + jnp.log(total)
            weights.append(exps.astype(jnp.bfloat16))
            shares.append(1.0 / total)
        out = jnp.dot(values, jnp.concatenate(weights, 1), preferred_element_type=jnp.float32)
        outs = [out[:, g * WINDOW : (g + 1) * WINDOW] * shares[g] for g in range(grp)]
        col = pn + kv * grp * HD
        act[q_at, col : col + grp * HD] = jnp.concatenate(outs, 0).T.astype(jnp.bfloat16)

    late = jnp.where(c == 0, 0, n_blocks - 1)
    early = n_blocks - 1 - late

    def attend_early(kv):
        for i in range(1, n_blocks - 1):
            attend(kv, i)
        attend(kv, early)

    def queries(kv, g):
        for low in range(0, rows, hrow):
            both = project(g, low)
            for col in range(0, gw, 128):
                at_col = kv * gw + col
                qrot[pl.ds(low, hrow), at_col : at_col + 128] = turn(
                    both[:, col : col + 128], low, HD ** -0.5
                )

    @pl.when(crossed)
    def _():
        remote(sink_own, sinkb, m_send.at[1], m_recv.at[1], partner).wait_recv()

    def pool(i):
        q_at = pl.ds(pl.multiple_of(i * WINDOW, WINDOW), WINDOW)
        window = pl.ds(pl.multiple_of(i * WINDOW, WINDOW), span)
        own_at = pl.ds(pl.multiple_of((i + 1) * WINDOW, WINDOW), WINDOW)
        band = inside_of(i) & (apart >= WINDOW - half_width) & (apart < WINDOW + half_width)
        band_f = band.astype(jnp.float32)
        counted = jnp.sum(band_f, -1, keepdims=True)
        summed = jnp.dot(
            band_f.astype(jnp.bfloat16),
            ext[window, gw : gw + pn],
            preferred_element_type=jnp.float32,
        )
        own_pool = ext[own_at, gw : gw + pn]
        pooled = (summed / counted - own_pool.astype(jnp.float32)).astype(jnp.bfloat16)
        act[q_at, 0:pn] = jnp.dot(
            pooled, mixb[...], preferred_element_type=jnp.float32
        ).astype(jnp.bfloat16)

    halo_wait(1, True)

    @pl.when(straight)
    def _():
        mix_local.wait()

    @pl.when(crossed)
    def _():
        mix_swap.wait_recv()

    for i in range(1, n_blocks - 1):
        pool(i)
    pool(early)

    stage(nz + 2, nz + 4, outer)
    gathered(2)
    queries(0, 2)
    halo_wait(0, True)
    own_out(middle, True, (0, 1), False)
    attend_early(0)
    own_out(middle, False, (0, 1), True)
    stage(nz + 4, nz + 2 * groups, outer)
    halo_wait(0, False)
    attend(0, late)
    halo_wait(1, False)
    pool(late)

    x_first = ((0, HALVES - 1), (2, 0))

    def side_of(block):
        return block // per_owner // CORES

    def r1_copy(block, h, rh, turned):
        take = pl.ds(rh * hrow, hrow)
        return remote(
            part.at[h, block, take],
            rs1.at[h, block, take],
            r1_send.at[h, int(turned)],
            r1_recv.at[h, block, rh],
            at(z, y, 1 - x, c) if turned else at(z, 1 - y, x, c),
        )

    def r2_copy(block, h, rh, turned):
        take = pl.ds(rh * hrow, hrow)
        owner = block // per_owner
        slot = block % per_owner
        side = jnp.where(straight if turned else side_of(block) == x, 0, 1)
        return remote(
            tot.at[h, block, take],
            fin.at[side, h, slot, take],
            r2_send.at[h, int(turned)],
            r2_recv.at[side],
            (z * NY + c, owner),
        )

    def each_block(d, lead, body):
        parity = y if lead == 0 else 1 - y
        for way in range(1 if d == 0 else 2):
            source = z + (2 * way - 1) * d

            @pl.when((source >= 0) & (source < nz))
            def _():
                body(source * NY + parity)

    def compute(d, h, lead, halves=(0, 1)):
        def body(block):
            if halves[0] == 0:

                @pl.when(crossed if lead == 0 else straight)
                def _():
                    w_copy(groups + h, block, 2).wait_recv()

            take = pl.ds(halves[0] * hrow, len(halves) * hrow)
            part[h, block, take] = jnp.dot(
                act[take], wo[block, h], preferred_element_type=jnp.float32
            ).astype(jnp.bfloat16)

            turned = (d, h) in x_first

            @pl.when(side_of(block) != x if turned else crossed)
            def _():
                for rh in halves:
                    r1_copy(block, h, rh, turned).start()

        each_block(d, lead, body)

    def join(d, h):
        turned = (d, h) in x_first

        def meet(block):
            for rh in range(2):
                take = pl.ds(rh * hrow, hrow)
                r1_copy(block, h, rh, turned).wait_recv()
                tot[h, block, take] = (
                    part[h, block, take].astype(jnp.float32)
                    + rs1[h, block, take].astype(jnp.float32)
                ).astype(jnp.bfloat16)

                @pl.when(crossed | (block // per_owner != tp))
                def _():
                    r2_copy(block, h, rh, turned).start()

        def body(block):
            @pl.when(side_of(block) == x if turned else straight)
            def _():
                meet(block)

        for lead in range(2):
            each_block(d, lead, body)

    gathered(3)
    queries(1, 3)
    log_swap = remote(log_own, log_in, m_send.at[2], m_recv.at[2], partner)

    for rh in range(2):
        for i in range(rh * n_blocks // 2, (rh + 1) * n_blocks // 2):
            attend(1, i)
        for h in range(HALVES):
            for lead in range(2):
                compute(0, h, lead, (rh,))

    @pl.when(crossed)
    def _():
        log_swap.start()

    def pass_on(d, h, ok):
        @pl.when(ok)
        def _():
            relay(d, groups + h)

    order = [(d, h) for d in range(nz) for h in range(HALVES)]

    def advance(n):
        d, h = order[n]
        compute(d, h, 0)
        pass_on(d, h, outer & crossed)
        if n + 1 < len(order):
            pass_on(*order[n + 1], outer & straight)
        compute(d, h, 1)

    for h in range(HALVES):
        pass_on(1, h, middle)
    for n in range(HALVES, len(order)):
        if n == HALVES:
            pass_on(*order[n], outer & straight)
        advance(n)
        if n == 2 * HALVES - 1:
            join(*order[0])
            for far in range(2, nz):
                for h in range(HALVES):
                    pass_on(far, h, middle)
        for ready in {4: (1, 2, 3), 6: (4, 5)}.get(n, ()):
            join(*order[ready])
    for ready in (6, 7):
        join(*order[ready])

    @pl.when(straight)
    def _():
        log_ref[...] = log_own[...]

    @pl.when(crossed)
    def _():
        log_swap.wait_recv()
        log_ref[...] = log_in[...]

    arrived(fin.at[1], r2_recv.at[1])

    @pl.when(crossed)
    def _():
        arrived(fin.at[0], r2_recv.at[0])

    for slot in range(per_owner):
        for h in range(HALVES):
            low = (slot * HALVES + h) * ohalf
            far = fin[1, h, slot].astype(jnp.float32)

            @pl.when(straight)
            def _():
                near = tot[h, tp * per_owner + slot].astype(jnp.float32)
                mixed_ref[:, low : low + ohalf] = (near + far).astype(jnp.bfloat16)

            @pl.when(crossed)
            def _():
                near = fin[0, h, slot].astype(jnp.float32)
                mixed_ref[:, low : low + ohalf] = (near + far).astype(jnp.bfloat16)

    def all_sent(way, count):
        departed(wg.at[pl.ds(0, groups), pl.ds(0, count * brow)], w_send.at[way, 0])
        departed(wo.at[pl.ds(0, count)], w_send.at[way, 1])

    all_sent(2, nz)
    for count in range(1, nz):
        for way, passed in ((0, z + 1), (1, nz - z)):

            @pl.when(onward[way] & (passed == count))
            def _():
                all_sent(way, count)

    halo_send(0, done=True)
    halo_send(1, done=True)

    @pl.when(straight)
    def _():
        departed(xg.at[pl.ds(0, 2)], x_send.at[0])
        departed(xg.at[pl.ds(0, CORES), spans[0]], x_send.at[1])

    @pl.when(crossed)
    def _():
        departed(xg.at[pl.ds(0, 3)], x_send.at[0])
        departed(xg.at[pl.ds(0, CORES), spans[1]], x_send.at[1])
        departed(wg.at[pl.ds(0, groups), pl.ds(0, brow)], load_send.at[0])
        departed(wo.at[0], load_send.at[1])
        mix_swap.wait_send()
        sink_swap.wait_send()
        log_swap.wait_send()

    for d, h in x_first:
        across = z if d == 0 else (z + d) % nz
        owner = across * NY // per_owner
        facing = owner // CORES == x
        plain = nsp - NY

        def gone(ok, source, count, sem):
            @pl.when(ok)
            def _():
                departed(source.at[h, pl.ds(0, count)], sem)

        gone(jnp.logical_not(facing), part, NY, r1_send.at[h, 1])
        gone(facing & (crossed | (owner != tp)), tot, NY, r2_send.at[h, 1])
        gone(crossed, part, plain, r1_send.at[h, 0])
        gone(straight & (owner == tp), tot, plain, r2_send.at[h, 0])
        gone(straight & (owner != tp), tot, plain - per_owner, r2_send.at[h, 0])


def place_kernel(mixed_ref, log_ref, mixed_out, log_out, sems):
    copies = [
        pltpu.make_async_copy(mixed_ref, mixed_out, sems.at[0]),
        pltpu.make_async_copy(log_ref, log_out, sems.at[1]),
    ]
    for copy in copies:
        copy.start()
    for copy in copies:
        copy.wait()


def fused(
    nz,
    ntp,
    tokens,
    norm_gain,
    query_weight,
    key_weight,
    value_weight,
    pool_in_weight,
    pool_mix_weight,
    sink_logit,
    out_pool_weight,
    out_attn_weight,
):
    rows, width = tokens.shape
    nsp = nz * NY
    dim = width * ntp
    qn, kn, pn = query_weight.shape[1], key_weight.shape[1], pool_in_weight.shape[1]
    fan = out_pool_weight.shape[0] + out_attn_weight.shape[0]
    ohalf = out_pool_weight.shape[1] // HALVES
    heads = sink_logit.shape[0]
    gw = 2 * kn
    groups = (qn + 2 * kn + pn) // gw
    pieces = groups + HALVES
    hbm = pl.BlockSpec(memory_space=pl.ANY)
    vmem = pl.BlockSpec(memory_space=pltpu.VMEM)
    dma = pltpu.SemaphoreType.DMA
    bf16 = jnp.bfloat16
    f32 = jnp.float32
    per_owner = nsp // ntp
    outs = (
        jax.ShapeDtypeStruct((rows, width), bf16),
        jax.ShapeDtypeStruct((heads, rows), f32),
    )
    mixed, logs = pl.pallas_call(
        functools.partial(layer_kernel, nz, ntp),
        out_shape=outs,
        in_specs=[hbm] * 10,
        out_specs=(vmem, vmem),
        scratch_shapes=[
            pltpu.VMEM((ntp, rows, width), bf16),
            pltpu.VMEM((rows, dim), bf16),
            pltpu.VMEM((groups, dim, gw), bf16),
            pltpu.VMEM((nsp, HALVES, fan, ohalf), bf16),
            pltpu.VMEM((rows, qn), bf16),
            pltpu.VMEM((rows + 2 * WINDOW, gw + pn), bf16),
            pltpu.VMEM((rows, fan), bf16),
            pltpu.VMEM((HALVES, nsp, rows, ohalf), bf16),
            pltpu.VMEM((HALVES, nsp, rows, ohalf), bf16),
            pltpu.VMEM((HALVES, nsp, rows, ohalf), bf16),
            pltpu.VMEM((2, HALVES, per_owner, rows, ohalf), bf16),
            pltpu.VMEM((rows, 128), f32),
            pltpu.VMEM((rows, 128), f32),
            pltpu.VMEM((pn, pn), bf16),
            pltpu.VMEM((1, dim), f32),
            pltpu.SMEM((heads,), f32),
            pltpu.VMEM((heads, 128), f32),
            pltpu.VMEM((heads, 128), f32),
            pltpu.VMEM((heads, rows), f32),
            pltpu.VMEM((heads, rows), f32),
            dma((2,)),
            dma((pieces,)),
            dma((3, 2)),
            dma((pieces, nz)),
            dma((groups,)),
            dma((HALVES, nz)),
            dma,
            dma((2,)),
            dma((ntp, 2)),
            dma((2,)),
            dma((3,)),
            dma((3,)),
            dma((2, 2)),
            dma((2, 2)),
            dma((HALVES, 2)),
            dma((HALVES, nsp, 2)),
            dma((HALVES, 2)),
            dma((2,)),
        ],
        compiler_params=pltpu.CompilerParams(
            collective_id=0, has_side_effects=True, vmem_limit_bytes=56 << 20
        ),
    )(
        tokens,
        norm_gain[None, :],
        query_weight,
        key_weight,
        value_weight,
        pool_in_weight,
        pool_mix_weight,
        sink_logit,
        out_pool_weight,
        out_attn_weight,
    )
    return pl.pallas_call(
        place_kernel,
        out_shape=outs,
        in_specs=[vmem, vmem],
        out_specs=(hbm, hbm),
        scratch_shapes=[dma((2,))],
    )(mixed, logs)


def choose(mesh):
    nsp, ntp = mesh.shape["sp"], mesh.shape["tp"]

    def body(*args):
        rows = args[0].shape[0]
        qn, kn, pn = args[2].shape[1], args[3].shape[1], args[5].shape[1]
        columns = args[8].shape[1]
        grid = nsp == 4 * NY and ntp == NX * CORES and nsp == NY * ntp
        cuts = columns % (HALVES * 128) == 0 and rows % (4 * WINDOW) == 0
        even = kn == 2 * HD and kn % 128 == 0 and qn == 4 * kn and pn == 2 * kn
        if grid and cuts and even:
            return fused(nsp // NY, ntp, *args)
        return local(*args)

    return body


def solution(mesh):
    return jax.shard_map(
        choose(mesh),
        mesh=mesh,
        in_specs=(
            P("sp", "tp"),
            P(),
            P("sp", "tp"),
            P("sp", "tp"),
            P("sp", "tp"),
            P("sp", "tp"),
            P("tp", None, None),
            P("tp"),
            P("tp", "sp"),
            P("tp", "sp"),
        ),
        out_specs=(P("sp", "tp"), P("tp", "sp")),
        check_vma=False,
    )
```
